256 devices in a mesh: ep: 16 (over y, x), tp: 16 (over z, core).
Axes of the slice: x: 4, y: 4, z: 8, core: 2. Of those that a mesh axis runs over, the one named last changes fastest.
Arguments:
- q_latent: bfloat16 [12288, 384], P(('ep', 'tp')), may hold values from -6 to 6
- kv_latent: bfloat16 [12288, 256], P(('ep', 'tp')), may hold values from -6 to 6
- rope_key: bfloat16 [12288, 64], P(('ep', 'tp')), may hold values from -6 to 6
- q_latent_gain: float32 [384], replicated, may hold values from 0.1 to 1.9
- kv_latent_gain: float32 [256], replicated, may hold values from 0.1 to 1.9
- w_query: bfloat16 [384, 3072], P(None, 'tp'), may hold values from -0.3125 to 0.3125
- w_key: bfloat16 [256, 2048], P(None, 'tp'), may hold values from -0.375 to 0.375
- w_value: bfloat16 [256, 2048], P(None, 'tp'), may hold values from -0.375 to 0.375
- query_gain: float32 [192], replicated, may hold values from 0.1 to 1.9
- key_gain: float32 [192], replicated, may hold values from 0.1 to 1.9
- w_mix: bfloat16 [2048, 2048], P('tp'), may hold values from -3 to 3
- tokens_b: bfloat16 [12288, 2048], P(('ep', 'tp')), may hold values from -6 to 6
- norm_gain: float32 [2048], replicated, may hold values from 0.1 to 1.9
- expert_ids: int32 [12288, 2], P(('ep', 'tp')), may hold values from 0 to 31, all different within a row; in each aligned block of 48 rows (0 to 47, 48 to 95, ...) at most 4 rows name the same one
- route_weights: float32 [12288, 2], P(('ep', 'tp')), may hold values from 0.05 to 1
- w_gate: bfloat16 [32, 2048, 4096], P('ep', None, 'tp'), may hold values from -0.125 to 0.125
- w_up: bfloat16 [32, 2048, 4096], P('ep', None, 'tp'), may hold values from -0.125 to 0.125
- w_down: bfloat16 [32, 4096, 2048], P('ep', 'tp'), may hold values from -0.09375 to 0.09375
Outputs:
- mix_out: bfloat16 [12288, 2048], P(('ep', 'tp'))
- expert_out: bfloat16 [12288, 2048], P(('ep', 'tp'))
The draws below stay inside these ranges and needn't reach their ends.
Inputs may be any that keep to these rules, and one draw needn't show every extreme that they name: `expert_ids`: each row names 2 different experts. Within the rows of one device, no expert is named more than 4 times, a bound that some block reaches.
All inputs are finite; a program needn't handle non-finite values.
Results may differ from the reference program's by a relative error of at most 0.018.
Values may be sent and summed in bfloat16 or wider, within the bound.
A program may use at most 192 MiB of HBM per device.

```python
import math
import jax
import jax.numpy as jnp
import numpy as np
from jax import lax

MODEL_DIM = 2048
HEADS = 16
Q_RANK = 384
KV_RANK = 256
NOPE_DIM = 128
ROPE_DIM = 64
VALUE_DIM = 128
EXPERTS = 32
FF_DIM = 4096
TOP_K = 2
ROWS = 768
TOKENS = 12288
CAP_SLOTS = 4
N_EP = 16
N_TP = 16


def levels(key, shape, shards, low, top_value):
    factor_of, own = 1.0, jax.random.fold_in(key, 6)
    for position, parts in shards:
        draws = jnp.exp(jax.random.uniform(jax.random.fold_in(own, position), (parts,), jnp.float32, low / len(shards), top_value / len(shards)))
        factor_of = factor_of * jnp.repeat(draws, shape[position] // parts).reshape([-1 if axis == position else 1 for axis in range(len(shape))])
    return factor_of


def deal_out(stream_key, own, number, rows, count, top, bound, lean):
    sequence = jax.random.permutation(stream_key, count)
    heavy_load, common = shares(count, rows * top, bound, lean, True), shares(count, rows * top, bound, lean, False)
    places = jnp.arange(count)

    def named(sizes, offset_by):
        used = int((sizes > 0).sum())
        fixed = max(1, used // 4)
        moved = fixed + (places - fixed + offset_by * (used - fixed)) % max(1, count - fixed)
        return jnp.zeros((count,), jnp.int32).at[sequence[jnp.where(places < fixed, places, moved)]].set(jnp.asarray(sizes, jnp.int32))

    sizes = jnp.where(number % 4 == 0, named(heavy_load, number // 4), named(common, number - number // 4 - 1))
    mixed = jax.random.permutation(jax.random.fold_in(own, 3), count)
    donor, sink = mixed[0:count // 2 * 2:2], mixed[1:count // 2 * 2:2]
    margin = jnp.minimum(sizes[donor] - 1, bound - sizes[sink]) // 2
    margin = jnp.where((donor == sequence[0]) | (sink == sequence[0]) | (sizes[sink] == 0), 0, jnp.maximum(margin, 0))
    moved = jax.random.randint(jax.random.fold_in(own, 4), (count // 2,), 0, 1 << 20) % (margin + 1)
    sizes = sizes.at[donor].add(-moved).at[sink].add(moved)
    members = jnp.searchsorted(jnp.cumsum(sizes), jnp.arange(rows * top), side="right").astype(jnp.int32)
    grid = members.reshape(top, rows).T
    grid = grid[jax.random.permutation(jax.random.fold_in(own, 1), rows)]
    offset_by = jax.random.randint(jax.random.fold_in(own, 2), (rows, 1), 0, top)
    return jnp.take_along_axis(grid, (jnp.arange(top)[None, :] + offset_by) % top, axis=1)


def shares(amount, total, reach, lean, full):
    portions = [(1 << 20) // math.isqrt(grade ** lean) + 1 for grade in range(1, amount + 1)]
    largest = reach if full else min(reach, max(-(-total // amount), total * portions[0] // sum(portions)))
    least = 1 if total - largest >= amount - 1 else 0
    counts, spare = [largest] + [least] * (amount - 1), total - largest - least * (amount - 1)
    while spare > 0:
        movable = [i for i in range(1, amount) if counts[i] < largest] or [i for i in range(1, amount) if counts[i] < reach]
        whole, left = sum([portions[i] for i in movable]), spare
        for i in movable:
            extra = min(reach - counts[i], max(1, left * portions[i] // whole), spare)
            counts[i] = counts[i] + extra
            spare = spare - extra
    return np.array(counts)


def noise(rng, shape, width, reach, split=(), kind=jnp.bfloat16):
    values = jax.random.normal(rng, shape, jnp.float32) * width
    if len(split) > 0:
        values = levels(rng, shape, split, -0.22, 0.18) * values
    return jnp.clip(values, min=-reach, max=reach).astype(kind)


def setup_inputs(seed: int = 0) -> dict:
    splits = jax.random.split(jax.random.key(seed), 19)
    q_latent = noise(splits[0], (TOKENS, Q_RANK), 1.0, 6.0, ((0, 256),))
    kv_latent = noise(splits[1], (TOKENS, KV_RANK), 1.0, 6.0, ((0, 256),))
    rope_key = noise(splits[2], (TOKENS, ROPE_DIM), 1.0, 6.0, ((0, 256),))
    q_latent_gain = jnp.clip(1.0 + 0.18 * jax.random.normal(splits[3], (Q_RANK,), jnp.float32), 0.1, 1.9)
    kv_latent_gain = jnp.clip(1.0 + 0.18 * jax.random.normal(splits[4], (KV_RANK,), jnp.float32), 0.1, 1.9)
    w_query = noise(splits[5], (Q_RANK, HEADS * (NOPE_DIM + ROPE_DIM)), Q_RANK ** -0.5, 0.3125, ((1, 16),))
    w_key = noise(splits[6], (KV_RANK, HEADS * NOPE_DIM), KV_RANK ** -0.5, 0.375, ((1, 16),))
    w_value = noise(splits[7], (KV_RANK, HEADS * VALUE_DIM), KV_RANK ** -0.5, 0.375, ((1, 16),))
    query_gain = jnp.clip(1.0 + 0.18 * jax.random.normal(splits[8], (NOPE_DIM + ROPE_DIM,), jnp.float32), 0.1, 1.9)
    key_gain = jnp.clip(1.0 + 0.18 * jax.random.normal(splits[9], (NOPE_DIM + ROPE_DIM,), jnp.float32), 0.1, 1.9)
    w_mix = noise(splits[10], (HEADS * VALUE_DIM, MODEL_DIM), 0.5, 3.0, ((0, 16),))
    tokens_b = noise(splits[11], (TOKENS, MODEL_DIM), 1.0, 6.0, ((0, 256),))
    norm_gain = jnp.clip(1.0 + 0.18 * jax.random.normal(splits[12], (MODEL_DIM,), jnp.float32), 0.1, 1.9)
    expert_ids_keys = jax.random.split(jax.random.fold_in(splits[13], 1), TOKENS // (ROWS // N_TP))
    expert_ids_turns = jax.random.permutation(jax.random.fold_in(splits[13], 3), TOKENS // (ROWS // N_TP))
    expert_ids = jax.vmap(lambda own, number: deal_out(jax.random.fold_in(splits[13], 2), own, number, ROWS // N_TP, EXPERTS, TOP_K, CAP_SLOTS, 1))(expert_ids_keys, expert_ids_turns).reshape((TOKENS, TOP_K))
    route_weights = jnp.clip(jnp.exp(math.log(1.0) - 2.9957323 * jax.random.uniform(splits[14], (TOKENS, TOP_K), jnp.float32) ** levels(splits[14], (TOKENS, TOP_K), ((0, 256),), -0.2, 0.2)), 0.05, 1.0)
    w_gate = noise(splits[15], (EXPERTS, MODEL_DIM, FF_DIM), MODEL_DIM ** -0.5, 0.125, ((0, 16), (2, 16)))
    w_up = noise(splits[16], (EXPERTS, MODEL_DIM, FF_DIM), MODEL_DIM ** -0.5, 0.125, ((0, 16), (2, 16)))
    w_down = noise(splits[17], (EXPERTS, FF_DIM, MODEL_DIM), FF_DIM ** -0.5, 0.09375, ((0, 16), (1, 16)))
    return {"q_latent": q_latent, "kv_latent": kv_latent, "rope_key": rope_key, "q_latent_gain": q_latent_gain, "kv_latent_gain": kv_latent_gain, "w_query": w_query, "w_key": w_key, "w_value": w_value, "query_gain": query_gain, "key_gain": key_gain, "w_mix": w_mix, "tokens_b": tokens_b, "norm_gain": norm_gain, "expert_ids": expert_ids, "route_weights": route_weights, "w_gate": w_gate, "w_up": w_up, "w_down": w_down}


EPSILON = 1e-06
THETA = 10000.0

def rms_scale(values, gains):
    return values * lax.rsqrt(lax.optimization_barrier(jnp.mean(values * values, axis=-1, keepdims=True)) + EPSILON) * gains

def rotate(values, positions):
    half_dim = values.shape[-1] // 2
    inverse = THETA ** (-jnp.arange(0, 2 * half_dim, 2, dtype=jnp.float32) / (2 * half_dim))
    angles = positions.astype(jnp.float32)[:, None] * inverse[None, :]
    view_shape = (positions.shape[0],) + (1,) * (values.ndim - 2) + (half_dim,)
    cosine = jnp.cos(angles).reshape(view_shape)
    sine_part = jnp.sin(angles).reshape(view_shape)
    first_half = values[..., :half_dim]
    second = values[..., half_dim:]
    return jnp.concatenate([first_half * cosine - second * sine_part, second * cosine + first_half * sine_part], axis=-1)

def reference(q_latent, kv_latent, rope_key, q_latent_gain, kv_latent_gain, w_query, w_key, w_value, query_gain, key_gain, w_mix, tokens_b, norm_gain, expert_ids, route_weights, w_gate, w_up, w_down):
    q_normed = rms_scale(q_latent.astype(jnp.float32), q_latent_gain).astype(jnp.bfloat16)
    kv_normed = rms_scale(kv_latent.astype(jnp.float32), kv_latent_gain).astype(jnp.bfloat16)
    positions = jnp.arange(TOKENS, dtype=jnp.int32)
    head_q = jnp.moveaxis(w_query.reshape(Q_RANK, HEADS, NOPE_DIM + ROPE_DIM), 1, 0)
    head_k = jnp.moveaxis(w_key.reshape(KV_RANK, HEADS, NOPE_DIM), 1, 0)
    head_v = jnp.moveaxis(w_value.reshape(KV_RANK, HEADS, VALUE_DIM), 1, 0)
    shared = rope_key.astype(jnp.float32)
    score_scale = (NOPE_DIM + ROPE_DIM) ** (-0.5)

    def one_head(head_weights):
        weight_q, weight_k, weight_v = head_weights
        queries = rms_scale(jnp.dot(q_normed, weight_q, preferred_element_type=jnp.float32), query_gain)
        queries = jnp.concatenate([queries[:, :NOPE_DIM], rotate(queries[:, NOPE_DIM:], positions)], axis=-1).astype(jnp.bfloat16)
        keys = jnp.concatenate([jnp.dot(kv_normed, weight_k, preferred_element_type=jnp.float32), shared], axis=-1)
        keys = rms_scale(keys, key_gain)
        keys = jnp.concatenate([keys[:, :NOPE_DIM], rotate(keys[:, NOPE_DIM:], positions)], axis=-1).astype(jnp.bfloat16)
        values = jnp.dot(kv_normed, weight_v, preferred_element_type=jnp.float32).astype(jnp.bfloat16)

        def query_block(row_data):
            scores = jnp.dot(row_data, keys.T, preferred_element_type=jnp.float32) * score_scale
            probs_f = jnp.exp(scores)
            totals = lax.optimization_barrier(jnp.sum(probs_f, axis=-1, keepdims=True))
            mixed = jnp.dot(probs_f.astype(jnp.bfloat16), values, preferred_element_type=jnp.float32)
            return (mixed / totals).astype(jnp.bfloat16)
        blocks = lax.map(query_block, queries.reshape(N_EP, ROWS, NOPE_DIM + ROPE_DIM))
        return blocks.reshape(TOKENS, VALUE_DIM)
    head_out = lax.map(one_head, (head_q, head_k, head_v))
    per_group = HEADS // N_TP
    mixed_sum = jnp.zeros((TOKENS, MODEL_DIM), jnp.float32)
    for group_index in range(N_TP):
        group_heads = jnp.moveaxis(head_out[group_index * per_group:(group_index + 1) * per_group], 0, 1)
        group_heads = group_heads.reshape(TOKENS, per_group * VALUE_DIM)
        rows_w = w_mix[group_index * per_group * VALUE_DIM:(group_index + 1) * per_group * VALUE_DIM]
        partial_value = lax.optimization_barrier(jnp.dot(group_heads, rows_w, preferred_element_type=jnp.float32).astype(jnp.bfloat16))
        mixed_sum = mixed_sum + partial_value.astype(jnp.float32)
    mix_out = mixed_sum.astype(jnp.bfloat16)
    b_normed = rms_scale(tokens_b.astype(jnp.float32), norm_gain).astype(jnp.bfloat16)
    flat_ids = expert_ids.reshape(-1)
    flat_weights = route_weights.reshape(-1)
    max_rows = N_EP * N_TP * CAP_SLOTS
    hidden_dim = FF_DIM // N_TP

    def one_expert(totals, expert):
        chosen = flat_ids == expert
        picked = jnp.nonzero(chosen, size=max_rows, fill_value=0)[0]
        is_live = jnp.arange(max_rows) < jnp.sum(chosen.astype(jnp.int32))
        owners = picked // TOP_K
        row_data = b_normed[owners]
        gate_pre = jnp.dot(row_data, w_gate[expert], preferred_element_type=jnp.float32)
        up_pre = jnp.dot(row_data, w_up[expert], preferred_element_type=jnp.float32)
        hidden = (jax.nn.silu(gate_pre) * up_pre).astype(jnp.bfloat16)
        partial_value = jnp.einsum('rtf,tfd->trd', hidden.reshape(max_rows, N_TP, hidden_dim).astype(jnp.float32), w_down[expert].reshape(N_TP, hidden_dim, MODEL_DIM).astype(jnp.float32))
        rounded = lax.optimization_barrier(partial_value.astype(jnp.bfloat16))
        result = lax.optimization_barrier(jnp.sum(rounded.astype(jnp.float32), axis=0)).astype(jnp.bfloat16)
        scaled = jnp.where(is_live, flat_weights[picked], 0.0)
        return (totals.at[owners].add(scaled[:, None] * result.astype(jnp.float32)), None)
    totals, _ = lax.scan(one_expert, jnp.zeros((TOKENS, MODEL_DIM), jnp.float32), jnp.arange(EXPERTS, dtype=jnp.int32))
    return (mix_out, totals.astype(jnp.bfloat16))
```

```python
import jax
import jax.numpy as jnp
import numpy as np
from jax import lax
from jax.experimental import pallas as pl
from jax.experimental.pallas import tpu as pltpu
from jax.sharding import PartitionSpec as P

F32, BF16 = jnp.float32, jnp.bfloat16
MESH = pl.DeviceIdType.MESH
EPSILON = 1e-06
THETA = 10000.0
LOG2E = 1.4426950408889634
SCORE = 192 ** (-0.5)
NT = (((1,), (1,)), ((), ()))
TN = (((0,), (0,)), ((), ()))
HALF = 64


def rope_tables():
    inverse = THETA ** (-np.arange(0, 64, 2, dtype=np.float64) / 64)
    rows = np.arange(768).reshape(8, 2, 48).transpose(1, 0, 2).reshape(768)
    angle = np.tile(rows[:, None] * inverse[None, :], (1, 2))
    base = np.concatenate([np.cos(angle), np.sin(angle)], axis=1).astype(np.float32)
    offset = np.tile((np.arange(16) * 768)[:, None] * inverse[None, :], (1, 4))
    shift = np.stack([np.cos(offset), np.sin(offset)], axis=1).astype(np.float32)
    return base.reshape(16, 48, 128), shift.reshape(16, 2, 128)


def send(src, dst, send_sem, recv_sem, device):
    pltpu.make_async_remote_copy(
        src_ref=src, dst_ref=dst, send_sem=send_sem, recv_sem=recv_sem, device_id=device, device_id_type=MESH
    ).start()


def await_bytes(ref, sem):
    pltpu.make_async_copy(ref, ref, sem).wait()


def normed(x, gain):
    return x * lax.rsqrt(jnp.mean(x * x, axis=-1, keepdims=True) + EPSILON) * gain


def layer(
    ql_ref, kvl_ref, rope_ref, vec_ref, wq_ref, wkv_ref, tokens_ref, ids_ref, route_ref, base_ref, shift_ref,
    wmix_hbm, wg_hbm, wu_hbm, wd_hbm,
    mix_ref, expert_ref,
    wmix, wg, wu, wd, qg, queries, acc, lg, st, outgoing, arrived, returned, xg, pg, sg, rr, rl, mp, msg, mr, ml,
    w_sem, z_sem, q_sib, la, lb, ls, a2a, ret, xr, xl, xs_own, xs_r, xs_l, sgs, rrs, rls, ms, mrs, mls, out_sem,
):
    e, t = lax.axis_index("ep"), lax.axis_index("tp")
    z, c = t // 2, t % 2
    other = 1 - c
    sib = (e, z * 2 + other)

    def zpeer(d):
        return (e, ((z + d) % 8) * 2 + c)

    right, left = zpeer(1), zpeer(7)
    ey, ex = e // 4, e % 4
    pa = other * ex + c * ey
    pb = other * ey + c * ex

    def origin(da, db):
        a, b = (pa + da + 4) % 4, (pb + db + 4) % 4
        return other * (b * 4 + a) + c * (a * 4 + b)

    barrier = pltpu.get_barrier_semaphore()
    for d in range(1, 8):
        pl.semaphore_signal(barrier, inc=1, device_id=zpeer(d), device_id_type=MESH)
    for d in range(1, 16):
        pl.semaphore_signal(barrier, inc=1, device_id=((e + d) % 16, t), device_id_type=MESH)
    pl.semaphore_signal(barrier, inc=1, device_id=sib, device_id_type=MESH)

    loads = [
        pltpu.make_async_copy(src, dst, w_sem.at[n])
        for n, (src, dst) in enumerate([(wg_hbm, wg), (wu_hbm, wu), (wd_hbm, wd), (wmix_hbm, wmix)])
    ]
    for load in loads:
        load.start()

    ids = ids_ref[...]
    experts = lax.broadcasted_iota(jnp.int32, (48, 32), 1)
    hot = [(ids[:, k : k + 1] == experts).astype(F32) for k in range(2)]
    lower = (
        lax.broadcasted_iota(jnp.int32, (48, 48), 0) > lax.broadcasted_iota(jnp.int32, (48, 48), 1)
    ).astype(BF16)
    before = [jnp.dot(lower, h.astype(BF16), preferred_element_type=F32) for h in hot]
    before[1] = before[1] + jnp.sum(hot[0], axis=0, keepdims=True)
    places = lax.broadcasted_iota(jnp.int32, (48, 128), 1).astype(F32)
    for k in range(2):
        rank = jnp.sum(hot[k] * before[k], axis=1, keepdims=True)
        slot = ids[:, k : k + 1].astype(F32) * 4.0 + rank
        st[k] = (slot == places).astype(BF16)
    b_normed = normed(tokens_ref[...].astype(F32), vec_ref[:, 1152:3200]).astype(BF16)
    slots = lax.dot_general(st[0] + st[1], b_normed, TN, preferred_element_type=F32)
    slots = slots.reshape(16, 8, 2048)
    outgoing[...] = jnp.concatenate([slots[:, :, :1024], slots[:, :, 1024:]], axis=1).astype(BF16)

    trig_q = shift_ref[pl.ds(e, 1), 0], shift_ref[pl.ds(e, 1), 1]
    lane = lax.broadcasted_iota(jnp.int32, (1, 128), 1)
    flip = jnp.where(lane < 64, -1.0, 1.0)

    def turning(u, gains):
        return (trig_q[0] * u + trig_q[1] * (pltpu.roll(u, 64, axis=1) * flip)) * gains

    def turned(v):
        return v + pltpu.roll(v, 64, axis=1)

    qg[c, z] = normed(ql_ref[...].astype(F32), vec_ref[:, 0:384]).astype(BF16)
    mine = lg.at[e * 2 + c, z]
    mine[:, 0:256] = normed(kvl_ref[...].astype(F32), vec_ref[:, 384:640]).astype(BF16)
    rope = rope_ref[...].astype(F32)
    rope_rot = turned(rope * turning(base_ref[c * 8 + z], vec_ref[:, 1024:1152]))
    squares = jnp.sum(jnp.where(lane < 64, rope * rope, 0.0), axis=1, keepdims=True)
    high = squares.astype(BF16).astype(F32)
    mine[:, 256:384] = jnp.where(
        lane < 64, rope_rot, jnp.where(lane == 64, high, jnp.where(lane == 65, squares - high, 0.0))
    ).astype(BF16)

    pl.semaphore_wait(barrier, 23)
    for d in range(1, 16):
        peer = (e + d) % 16
        send(outgoing.at[peer], arrived.at[e], out_sem.at[0], a2a, (peer, t))
    for d in range(1, 8):
        send(mine, mine, out_sem.at[1], z_sem.at[0], zpeer(d))
    for d in range(1, 8):
        send(qg.at[c, z], qg.at[c, z], out_sem.at[2], z_sem.at[1], zpeer(d))
    arrived[pl.ds(e, 1)] = outgoing[pl.ds(e, 1)]

    a_up, a_down = (origin(1, 0), t), (origin(-1, 0), t)
    b_up, b_down = (origin(0, 1), t), (origin(0, -1), t)

    def block(da, db):
        return lg.at[origin(da, db) * 2 + c]

    def part(da, db, n):
        return lg.at[origin(da, db) * 2 + c, pl.ds(4 * n, 4)]

    def full(ref, sem, device):
        send(ref, ref, out_sem.at[3], sem, device)

    def along_b(n, da):
        full(block(da, 0), lb.at[n, 0], b_up)
        full(block(da, 0), lb.at[n, 1], b_down)
        full(block(da, 0), ls, sib)

    def start_latents():
        await_bytes(lg.at[0, pl.ds(0, 7)], z_sem.at[0])
        full(block(0, 0), la.at[0], a_up)
        full(block(0, 0), la.at[1], a_down)
        along_b(0, 0)

    def relay_a():
        await_bytes(block(-1, 0), la.at[0])
        full(part(-1, 0, 0), la.at[2], a_up)
        along_b(1, -1)
        await_bytes(block(1, 0), la.at[1])
        full(part(1, 0, 1), la.at[3], a_down)
        along_b(2, 1)

    def relay_a_far():
        await_bytes(part(2, 0, 0), la.at[2])
        await_bytes(part(2, 0, 1), la.at[3])
        along_b(3, 2)

    def relay_b(n):
        da = (0, -1, 1, 2)[n]
        await_bytes(block(da, -1), lb.at[n, 0])
        full(part(da, -1, 0), lb.at[n, 2], b_up)
        full(block(da, -1), ls, sib)
        await_bytes(block(da, 1), lb.at[n, 1])
        full(part(da, 1, 1), lb.at[n, 3], b_down)
        full(block(da, 1), ls, sib)

    def relay_b_far(n):
        da = (0, -1, 1, 2)[n]
        await_bytes(part(da, 2, 0), lb.at[n, 2])
        await_bytes(part(da, 2, 1), lb.at[n, 3])
        full(block(da, 2), ls, sib)

    def start_queries():
        await_bytes(qg.at[0, pl.ds(0, 7)], z_sem.at[1])
        send(qg.at[c], qg.at[c], out_sem.at[4], q_sib, sib)

    def make_queries():
        await_bytes(qg.at[0], q_sib)

        def rows(n, carry):
            x = qg[n // 2, pl.ds((n % 2) * 4, 4)].reshape(192, 384)
            p = jnp.dot(x, wq_ref[...], preferred_element_type=F32)
            nope, rot = p[:, :128], p[:, 128:]
            total = jnp.sum(nope * nope + jnp.where(lane < 64, rot * rot, 0.0), axis=1, keepdims=True)
            scale = lax.rsqrt(total * (1.0 / 192.0) + EPSILON) * (SCORE * LOG2E)
            angles = turning(base_ref[pl.ds(n * 4, 4)].reshape(192, 128), vec_ref[:, 768:896])
            rot = jnp.where(lane < 64, turned(rot * angles), 0.0) * scale
            at = pl.ds(pl.multiple_of(n * 192, 192), 192)
            queries[at, 0:128] = (nope * vec_ref[:, 640:768] * scale).astype(BF16)
            queries[at, 128:256] = rot.astype(BF16)
            acc[at] = jnp.zeros((192, 256), F32)
            return carry

        lax.fori_loop(0, 4, rows, 0)

    def attend(first, last):
        def keys_of(n, carry):
            rows = lg[n].reshape(384, 384)
            kv = jnp.dot(rows[:, :256], wkv_ref[...], preferred_element_type=F32)
            tail = rows[:, 256:].astype(F32)
            nope = kv[:, :128]
            total = jnp.sum(nope * nope + jnp.where(lane < 64, 0.0, tail), axis=1, keepdims=True)
            scale = lax.rsqrt(total * (1.0 / 192.0) + EPSILON)
            keys = jnp.concatenate(
                [nope * (vec_ref[:, 896:1024] * scale), jnp.where(lane < 64, tail, 0.0) * scale], axis=1
            ).astype(BF16)
            values = jnp.concatenate([kv[:, 128:].astype(BF16), jnp.ones((384, 128), BF16)], axis=1)
            for m in range(3):
                at = pl.ds(m * 256, 256)
                scores = lax.dot_general(queries[at], keys, NT, preferred_element_type=F32)
                acc[at] += jnp.dot(jnp.exp2(scores).astype(BF16), values, preferred_element_type=F32)
            return carry

        lax.fori_loop(first, last, keys_of, 0)

    def xblock(zo, h, core):
        return xg.at[(zo * 2 + h) * 2 + core]

    def xsend(ref, sem, device):
        send(ref, ref, out_sem.at[5], sem, device)

    def settle():
        await_bytes(outgoing.at[pl.ds(0, 15)], a2a)
        row = lax.broadcasted_iota(jnp.int32, (128, 128), 0)
        col = lax.broadcasted_iota(jnp.int32, (128, 128), 1)
        moved = (row == (col % 8 // 4) * 64 + col // 8 * 4 + col % 4).astype(BF16)
        came = arrived[...].astype(F32)
        for n in range(2):
            piece = came[:, n * 8 : n * 8 + 8].reshape(128, 1024).astype(BF16)
            piece = jnp.dot(moved, piece, preferred_element_type=F32).astype(BF16)
            for h in range(2):
                xg[(z * 2 + h) * 2 + c, :, n * 1024 : n * 1024 + 1024] = piece[h * HALF : h * HALF + HALF]
        for h in range(2):
            xsend(xblock(z, h, c), xr.at[h], right)
            xsend(xblock(z, h, c), xl.at[h], left)
            xsend(xblock(z, h, c), xs_own.at[h], sib)

    def relay_rows(j):
        k, hr = j // 2 + 1, j % 2
        hl = hr + j // 6
        from_left, from_right = xblock((z - k + 8) % 8, hr, c), xblock((z + k) % 8, hl, c)
        await_bytes(from_left, xr.at[j])

        @pl.when(j <= 4)
        def _():
            xsend(from_left, xr.at[j + 2], right)

        xsend(from_left, xs_r.at[j], sib)
        await_bytes(from_right, xl.at[j])

        @pl.when(j <= 3)
        def _():
            xsend(from_right, xl.at[j + 2], left)

        @pl.when(j == 5)
        def _():
            xsend(from_right, xl.at[6], left)

        xsend(from_right, xs_l.at[j], sib)

    def expert(zo, h, sem):
        x = xg[pl.ds((zo * 2 + h) * 2, 2)].reshape(128, 2048)
        gate = jnp.dot(x, wg[h], preferred_element_type=F32)
        up = jnp.dot(x, wu[h], preferred_element_type=F32)
        hidden = (gate / (1.0 + jnp.exp(-gate)) * up).astype(BF16)
        for n in range(4):
            cols = pl.ds(n * 512, 512)
            y = jnp.dot(hidden, wd[h, :, cols], preferred_element_type=F32).astype(BF16)
            pg[zo * 2 + h, :, cols] = y[:HALF]
            pg[16 + zo * 2 + h, :, cols] = y[HALF:]
        send(pg.at[other * 16 + zo * 2 + h], sg.at[zo * 2 + h], out_sem.at[6], sem, sib)

    def expert_pair(i):
        j = i - 1
        k = (j + 2) // 2
        h0 = (1 - (i + 7) // 8) * 0 + ((i + 7) // 8) * (j + 2) % 2
        started = (i + 7) // 8

        @pl.when(i == 0)
        def _():
            await_bytes(xblock(z, 0, other), xs_own.at[0])
            await_bytes(xblock(z, 1, other), xs_own.at[1])

        @pl.when(i > 0)
        def _():
            await_bytes(xblock((z - k + 8) % 8, 0, other), xs_r.at[j])
            await_bytes(xblock((z + k) % 8, 0, other), xs_l.at[j])

        def one(s, carry):
            zo = (z + started * (s * k + (1 - s) * (8 - k))) % 8
            hs = (1 - started) * s + started * (h0 + s * (i // 7))
            expert(zo, hs, sgs.at[i * 2 + s])
            return carry

        lax.fori_loop(0, 2, one, 0)

    def add_rows(out, terms, rows):
        def tile(n, carry):
            at = pl.ds(pl.multiple_of(n * 16, 16), 16)
            total = terms[0][at].astype(F32)
            for term in terms[1:]:
                total += term[at].astype(F32)
            out[at] = total.astype(BF16)
            return carry

        lax.fori_loop(0, rows // 16, tile, 0)

    def sums_event(m):
        k = 4 - (m + 1) // 2
        for side in range(2):
            h = m % 2 if side == 0 else 1 - m % 2
            zo = (z + k) % 8 if side == 0 else (z + 8 - k) % 8
            step = 2 * (k - 1) + h + 1 if k < 4 else 7
            which = (1 - side) if k < 4 else side
            await_bytes(sg.at[zo * 2 + h], sgs.at[step * 2 + which])
            mine_, recv, sems, device = (pg.at[c * 16 + zo * 2 + h], (rr, rl)[side], (rrs, rls)[side], (right, left)[side])
            terms = [mine_, sg.at[zo * 2 + h]]
            if m >= 2:
                await_bytes(recv.at[m - 2], sems.at[m - 2])
                terms.append(recv.at[m - 2])
            add_rows(mine_, terms, HALF)
            send(mine_, recv.at[m], out_sem.at[7], sems.at[m], device)

    def sums_final():
        for h in range(2):
            await_bytes(sg.at[z * 2 + h], sgs.at[h])
            await_bytes(rr.at[6 - h], rrs.at[6 - h])
            await_bytes(rl.at[5 + h], rls.at[5 + h])
            own = pg.at[c * 16 + z * 2 + h]
            add_rows(own, [own, sg.at[z * 2 + h], rr.at[6 - h], rl.at[5 + h]], HALF)
        row = lax.broadcasted_iota(jnp.int32, (128, 128), 0)
        col = lax.broadcasted_iota(jnp.int32, (128, 128), 1)
        back = (col == (row % 8 // 4) * 64 + row // 8 * 4 + row % 4).astype(BF16)
        done = pg[pl.ds(c * 16 + z * 2, 2)].reshape(128, 2048)
        rows = jnp.dot(back, done, preferred_element_type=F32).reshape(16, 8, 2048)
        arrived[...] = jnp.concatenate([rows[:, :, :1024], rows[:, :, 1024:]], axis=1).astype(BF16)
        for d in range(1, 16):
            peer = (e + d) % 16
            send(arrived.at[peer], returned.at[e], out_sem.at[8], ret, (peer, t))
        returned[pl.ds(e, 1)] = arrived[pl.ds(e, 1)]

    def project():
        def piece(n, carry):
            core, quarter = n // 4, n % 4
            at = pl.ds(pl.multiple_of(core * 384, 384), 384)
            block_ = acc[at]
            heads = (block_[:, :128] / block_[:, 128:]).astype(BF16)
            y = jnp.dot(
                heads, wmix[:, pl.ds(pl.multiple_of(quarter * 512, 512), 512)], preferred_element_type=F32
            ).astype(BF16)
            for zo in range(8):
                mp[core * 16 + zo * 2 + quarter // 2, :, pl.ds(pl.multiple_of(quarter % 2 * 512, 512), 512)] = y[
                    zo * 48 : zo * 48 + 48
                ]
            return carry

        lax.fori_loop(0, 8, piece, 0)
        send(mp.at[pl.ds(other * 16, 16)], msg, out_sem.at[9], ms, sib)

    def mix_event(m):
        k = 4 - (m + 1) // 2
        if m == 0:
            await_bytes(msg, ms)
        for side in range(2):
            h = m % 2 if side == 0 else 1 - m % 2
            zo = (z + k) % 8 if side == 0 else (z + 8 - k) % 8
            mine_, recv, sems, device = (mp.at[c * 16 + zo * 2 + h], (mr, ml)[side], (mrs, mls)[side], (right, left)[side])
            terms = [mine_, msg.at[zo * 2 + h]]
            if m >= 2:
                await_bytes(recv.at[m - 2], sems.at[m - 2])
                terms.append(recv.at[m - 2])
            add_rows(mine_, terms, 48)
            send(mine_, recv.at[m], out_sem.at[10], sems.at[m], device)

    def mix_final():
        for h in range(2):
            await_bytes(mr.at[6 - h], mrs.at[6 - h])
            await_bytes(ml.at[5 + h], mls.at[5 + h])
            add_rows(
                mix_ref.at[:, pl.ds(h * 1024, 1024)],
                [mp.at[c * 16 + z * 2 + h], msg.at[z * 2 + h], mr.at[6 - h], ml.at[5 + h]],
                48,
            )

    def combine():
        await_bytes(outgoing.at[pl.ds(0, 15)], ret)
        came = returned[...].astype(F32)
        for n in range(2):
            piece = came[:, n * 8 : n * 8 + 8].reshape(128, 1024).astype(BF16)
            total = jnp.zeros((48, 1024), F32)
            for k in range(2):
                total += jnp.dot(st[k], piece, preferred_element_type=F32) * route_ref[:, k : k + 1]
            expert_ref[:, n * 1024 : n * 1024 + 1024] = total.astype(BF16)

    start_latents()
    start_queries()
    settle()
    for load in loads:
        load.wait()

    def step(i, carry):
        @pl.when(i == 0)
        def _():
            relay_a()
            make_queries()

        @pl.when(i > 0)
        def _():
            relay_rows(i - 1)

        @pl.when(i == 1)
        def _():
            relay_a_far()
            relay_b(0)

        @pl.when(i == 2)
        def _():
            relay_b_far(0)
            relay_b(1)

        @pl.when(i == 3)
        def _():
            relay_b_far(1)
            relay_b(2)

        @pl.when(i == 4)
        def _():
            relay_b_far(2)
            relay_b(3)

        @pl.when(i == 5)
        def _():
            relay_b_far(3)
            await_bytes(lg.at[pl.ds(0, 16)], ls)

        @pl.when(i > 0)
        def _():
            expert_pair(i - 1)

        @pl.when(i >= 6)
        def _():
            attend((i - 6) * 6, (i - 5) * 6)

        return carry

    lax.fori_loop(0, 8, step, 0)
    expert_pair(7)
    sums_event(0)
    sums_event(1)

    for m in range(2, 7):
        attend(12 + (m - 2) * 4, 12 + (m - 1) * 4)
        sums_event(m)
    project()
    mix_event(0)
    mix_event(1)
    sums_final()
    for m in range(2, 7):
        mix_event(m)
    combine()
    mix_final()

    await_bytes(outgoing.at[pl.ds(0, 15)], out_sem.at[0])
    await_bytes(lg.at[0, pl.ds(0, 7)], out_sem.at[1])
    await_bytes(qg.at[0, pl.ds(0, 7)], out_sem.at[2])
    await_bytes(lg.at[pl.ds(0, 31)], out_sem.at[3])
    await_bytes(qg.at[0], out_sem.at[4])
    await_bytes(xg.at[pl.ds(0, 30)], out_sem.at[5])
    await_bytes(xg.at[pl.ds(0, 16)], out_sem.at[6])
    await_bytes(xg.at[pl.ds(0, 14)], out_sem.at[7])
    await_bytes(outgoing.at[pl.ds(0, 15)], out_sem.at[8])
    await_bytes(msg, out_sem.at[9])
    await_bytes(mp.at[pl.ds(0, 14)], out_sem.at[10])


def on_device(
    q_latent, kv_latent, rope_key, q_latent_gain, kv_latent_gain, w_query, w_key, w_value, query_gain, key_gain,
    w_mix, tokens_b, norm_gain, expert_ids, route_weights, w_gate, w_up, w_down,
):
    base, shift = rope_tables()

    def turn_gain(g):
        return jnp.concatenate([g[128:192], -g[160:192], g[128:160]])

    vec = jnp.concatenate(
        [
            q_latent_gain, kv_latent_gain, query_gain[:128], turn_gain(query_gain), key_gain[:128], turn_gain(key_gain),
            norm_gain,
        ]
    )[None, :]
    wq = jnp.concatenate([w_query, w_query[:, 160:192], w_query[:, 128:160]], axis=1)
    wkv = jnp.concatenate([w_key, w_value], axis=1)
    rope = jnp.concatenate([rope_key, rope_key[:, 32:], rope_key[:, :32]], axis=1)
    vmem = pl.BlockSpec(memory_space=pltpu.VMEM)
    hbm = pl.BlockSpec(memory_space=pl.ANY)
    dma = pltpu.SemaphoreType.DMA
    out = jax.ShapeDtypeStruct((48, 2048), BF16)
    return pl.pallas_call(
        layer,
        out_shape=(out, out),
        in_specs=[vmem] * 11 + [hbm] * 4,
        out_specs=(vmem, vmem),
        scratch_shapes=[
            pltpu.VMEM((128, 2048), BF16),
            pltpu.VMEM((2, 2048, 256), BF16),
            pltpu.VMEM((2, 2048, 256), BF16),
            pltpu.VMEM((2, 256, 2048), BF16),
            pltpu.VMEM((2, 8, 48, 384), BF16),
            pltpu.VMEM((768, 256), BF16),
            pltpu.VMEM((768, 256), F32),
            pltpu.VMEM((32, 8, 48, 384), BF16),
            pltpu.VMEM((2, 48, 128), BF16),
            pltpu.VMEM((16, 16, 1024), BF16),
            pltpu.VMEM((16, 16, 1024), BF16),
            pltpu.VMEM((16, 16, 1024), BF16),
            pltpu.VMEM((32, HALF, 2048), BF16),
            pltpu.VMEM((32, HALF, 2048), BF16),
            pltpu.VMEM((16, HALF, 2048), BF16),
            pltpu.VMEM((7, HALF, 2048), BF16),
            pltpu.VMEM((7, HALF, 2048), BF16),
            pltpu.VMEM((32, 48, 1024), BF16),
            pltpu.VMEM((16, 48, 1024), BF16),
            pltpu.VMEM((7, 48, 1024), BF16),
            pltpu.VMEM((7, 48, 1024), BF16),
            dma((4,)),
            dma((2,)),
            dma,
            dma((4,)),
            dma((4, 4)),
            dma,
            dma,
            dma,
            dma((7,)),
            dma((7,)),
            dma((2,)),
            dma((7,)),
            dma((7,)),
            dma((16,)),
            dma((7,)),
            dma((7,)),
            dma,
            dma((7,)),
            dma((7,)),
            dma((11,)),
        ],
        compiler_params=pltpu.CompilerParams(
            collective_id=0, has_side_effects=True, vmem_limit_bytes=67_043_328
        ),
    )(
        q_latent, kv_latent, rope, vec, wq, wkv, tokens_b, expert_ids, route_weights, jnp.asarray(base), jnp.asarray(shift),
        w_mix, w_gate, w_up, w_down,
    )


def solution(mesh):
    rows, whole = P(("ep", "tp"), None), P()
    in_specs = (
        rows, rows, rows, whole, whole, P(None, "tp"), P(None, "tp"), P(None, "tp"), whole, whole, P("tp", None), rows,
        whole, rows, rows, P("ep", None, "tp"), P("ep", None, "tp"), P("ep", "tp", None),
    )
    return jax.shard_map(on_device, mesh=mesh, in_specs=in_specs, out_specs=(rows, rows), check_vma=False)
```

```python
import jax
import jax.numpy as jnp
import numpy as np
from jax import lax
from jax.experimental import pallas as pl
from jax.experimental.pallas import tpu as pltpu
from jax.sharding import PartitionSpec as P

F32, BF16 = jnp.float32, jnp.bfloat16
MESH = pl.DeviceIdType.MESH
EPSILON = 1e-06
THETA = 10000.0
LOG2E = 1.4426950408889634
SCORE = 192 ** (-0.5)
NT = (((1,), (1,)), ((), ()))
TN = (((0,), (0,)), ((), ()))
HALF = 64
OFFSETS = (
    (0, 0), (0, 1), (1, 0), (0, 3), (3, 0), (1, 1), (3, 3), (0, 2), (2, 0), (1, 3), (3, 1), (2, 1), (1, 2), (2, 3), (3, 2), (2, 2),
)


def rope_tables():
    inverse = THETA ** (-np.arange(0, 64, 2, dtype=np.float64) / 64)
    rows = np.arange(768).reshape(8, 2, 48).transpose(1, 0, 2).reshape(768)
    angle = np.tile(rows[:, None] * inverse[None, :], (1, 2))
    base = np.concatenate([np.cos(angle), np.sin(angle)], axis=1).astype(np.float32)
    offset = np.tile((np.arange(16) * 768)[:, None] * inverse[None, :], (1, 4))
    shift = np.stack([np.cos(offset), np.sin(offset)], axis=1).astype(np.float32)
    return base.reshape(16, 48, 128), shift.reshape(16, 2, 128)


def send(src, dst, send_sem, recv_sem, device):
    pltpu.make_async_remote_copy(
        src_ref=src, dst_ref=dst, send_sem=send_sem, recv_sem=recv_sem, device_id=device, device_id_type=MESH
    ).start()


def await_bytes(ref, sem):
    pltpu.make_async_copy(ref, ref, sem).wait()


def normed(x, gain):
    return x * lax.rsqrt(jnp.mean(x * x, axis=-1, keepdims=True) + EPSILON) * gain


def layer(
    *refs,
):
    inputs, (mix_ref, expert_ref), held = refs[:20], refs[20:22], refs[22:42]
    (
        tokens_ref, b_gain, ids_ref, ql_ref, kvl_ref, rope_ref, ql_gain, kvl_gain, q_gain, k_gain, base_ref, shift_ref,
        wq_ref, wk_ref, wv_ref, route_ref, wg, wu, wd, wmix,
    ) = held
    (
    wq, wkv, qg, queries, acc, lg, st, outgoing, arrived, returned, xg, pg, sg, rr, rl, mp, msg, mr, ml,
    w_sem, z_sem, qr, ql, q_sib, la, lb, ls, a2a, ret, xr, xl, xs_own, xs_r, xs_l, sgs, rrs, rls, ms, mrs, mls, out_sem,
    ) = refs[42:]
    e, t = lax.axis_index("ep"), lax.axis_index("tp")
    z, c = t // 2, t % 2
    other = 1 - c
    sib = (e, z * 2 + other)

    def zpeer(d):
        return (e, ((z + d) % 8) * 2 + c)

    right, left = zpeer(1), zpeer(7)
    ey, ex = e // 4, e % 4
    pa = other * ex + c * ey
    pb = other * ey + c * ex

    def away(n):
        dy, dx = OFFSETS[n]
        return ((ey + dy) % 4) * 4 + (ex + dx) % 4

    def back_from(n):
        dy, dx = OFFSETS[n]
        return ((ey + 4 - dy) % 4) * 4 + (ex + 4 - dx) % 4

    def origin(da, db):
        a, b = (pa + da + 4) % 4, (pb + db + 4) % 4
        return other * (b * 4 + a) + c * (a * 4 + b)

    barrier = pltpu.get_barrier_semaphore()
    for d in range(1, 8):
        pl.semaphore_signal(barrier, inc=1, device_id=zpeer(d), device_id_type=MESH)
    for d in range(1, 16):
        pl.semaphore_signal(barrier, inc=1, device_id=((e + d) % 16, t), device_id_type=MESH)
    pl.semaphore_signal(barrier, inc=1, device_id=sib, device_id_type=MESH)

    loads = [pltpu.make_async_copy(src, dst, w_sem.at[n]) for n, (src, dst) in enumerate(zip(inputs, held))]
    for load in loads[:12]:
        load.start()
    for load in loads[:3]:
        load.wait()

    row48 = lax.broadcasted_iota(jnp.int32, (48, 48), 0)
    col48 = lax.broadcasted_iota(jnp.int32, (48, 48), 1)

    def column(x):
        return jnp.sum(jnp.where(row48 == col48, x, 0.0), axis=1, keepdims=True)

    ids = [column(ids_ref[k : k + 1].astype(F32)) for k in range(2)]
    place32 = lax.broadcasted_iota(jnp.int32, (1, 32), 1)
    experts = place32 % 2 * 1.0
    for n in range(16):
        experts += jnp.where(place32 // 2 == n, (away(n) * 2).astype(F32), 0.0)
    first_slot = (place32 * 4).astype(F32)
    hot = [(ids[k] == experts).astype(F32) for k in range(2)]
    lower = (row48 > col48).astype(BF16)
    before = [jnp.dot(lower, h.astype(BF16), preferred_element_type=F32) for h in hot]
    before[1] = before[1] + jnp.sum(hot[0], axis=0, keepdims=True)
    places = lax.broadcasted_iota(jnp.int32, (48, 128), 1).astype(F32)
    for k in range(2):
        rank = jnp.sum(hot[k] * before[k], axis=1, keepdims=True)
        slot = jnp.sum(hot[k] * first_slot, axis=1, keepdims=True) + rank
        st[k] = (slot == places).astype(BF16)
    b_normed = normed(tokens_ref[...].astype(F32), b_gain[...].reshape(1, 2048)).astype(BF16)
    slots = lax.dot_general(st[0] + st[1], b_normed, TN, preferred_element_type=F32)
    slots = slots.reshape(16, 8, 2048)
    outgoing[...] = jnp.concatenate([slots[:, :, :1024], slots[:, :, 1024:]], axis=1).astype(BF16)

    for load in loads[12:]:
        load.start()
    for load in loads[3:12]:
        load.wait()

    trig_q = shift_ref[pl.ds(e, 1), 0], shift_ref[pl.ds(e, 1), 1]
    lane = lax.broadcasted_iota(jnp.int32, (1, 128), 1)
    flip = jnp.where(lane < 64, -1.0, 1.0)

    def turning(u, gains):
        return (trig_q[0] * u + trig_q[1] * (pltpu.roll(u, 64, axis=1) * flip)) * gains

    def swapped(v):
        return jnp.concatenate([v, v[:, 32:64], v[:, 0:32]], axis=1)

    def turn_gain(g):
        tail = g[:, 128:192]
        return swapped(tail) * jnp.where((lane >= 64) & (lane < 96), -1.0, 1.0)

    gq, kg = q_gain[...].reshape(1, 192), k_gain[...].reshape(1, 192)

    def turned(v):
        return v + pltpu.roll(v, 64, axis=1)

    qg[c, z] = normed(ql_ref[...].astype(F32), ql_gain[...].reshape(1, 384)).astype(BF16)
    mine = lg.at[e * 2 + c, z]
    mine[:, 0:256] = normed(kvl_ref[...].astype(F32), kvl_gain[...].reshape(1, 256)).astype(BF16)
    rope = swapped(rope_ref[...].astype(F32))
    rope_rot = turned(rope * turning(base_ref[c * 8 + z], turn_gain(kg)))
    squares = jnp.sum(jnp.where(lane < 64, rope * rope, 0.0), axis=1, keepdims=True)
    high = squares.astype(BF16).astype(F32)
    mine[:, 256:384] = jnp.where(
        lane < 64, rope_rot, jnp.where(lane == 64, high, jnp.where(lane == 65, squares - high, 0.0))
    ).astype(BF16)

    pl.semaphore_wait(barrier, 23)
    for n in range(1, 16):
        send(outgoing.at[n], arrived.at[n], out_sem.at[0], a2a.at[n // 8], (away(n), t))
    for d in range(1, 8):
        send(mine, mine, out_sem.at[1], z_sem, zpeer(d))
    arrived[0] = outgoing[0]

    a_up, a_down = (origin(1, 0), t), (origin(-1, 0), t)
    b_up, b_down = (origin(0, 1), t), (origin(0, -1), t)

    def block(da, db):
        return lg.at[origin(da, db) * 2 + c]

    def part(da, db, n):
        return lg.at[origin(da, db) * 2 + c, pl.ds(4 * n, 4)]

    def full(ref, sem, device):
        send(ref, ref, out_sem.at[3], sem, device)

    def along_b(n, da):
        full(block(da, 0), lb.at[n, 0], b_up)
        full(block(da, 0), lb.at[n, 1], b_down)
        full(block(da, 0), ls, sib)

    def start_latents():
        await_bytes(lg.at[0, pl.ds(0, 7)], z_sem)
        full(block(0, 0), la.at[0], a_up)
        full(block(0, 0), la.at[1], a_down)
        along_b(0, 0)

    def relay_a():
        await_bytes(block(-1, 0), la.at[0])
        full(part(-1, 0, 0), la.at[2], a_up)
        along_b(1, -1)
        await_bytes(block(1, 0), la.at[1])
        full(part(1, 0, 1), la.at[3], a_down)
        along_b(2, 1)

    def relay_a_far():
        await_bytes(part(2, 0, 0), la.at[2])
        await_bytes(part(2, 0, 1), la.at[3])
        along_b(3, 2)

    def relay_b(n):
        da = (0, -1, 1, 2)[n]
        await_bytes(block(da, -1), lb.at[n, 0])
        full(part(da, -1, 0), lb.at[n, 2], b_up)
        full(block(da, -1), ls, sib)
        await_bytes(block(da, 1), lb.at[n, 1])
        full(part(da, 1, 1), lb.at[n, 3], b_down)
        full(block(da, 1), ls, sib)

    def relay_b_far(n):
        da = (0, -1, 1, 2)[n]
        await_bytes(part(da, 2, 0), lb.at[n, 2])
        await_bytes(part(da, 2, 1), lb.at[n, 3])
        full(block(da, 2), ls, sib)

    def relay_queries(i):
        from_left, from_right = qg.at[c, (z + 8 - i) % 8], qg.at[c, (z + i) % 8]

        @pl.when((i >= 1) & (i <= 4))
        def _():
            await_bytes(from_left, qr.at[i - 1])

        @pl.when((i >= 1) & (i <= 3))
        def _():
            await_bytes(from_right, ql.at[i - 1])

        @pl.when(i <= 3)
        def _():
            send(from_left, from_left, out_sem.at[2], qr.at[i], right)

        @pl.when(i <= 2)
        def _():
            send(from_right, from_right, out_sem.at[2], ql.at[i], left)

        @pl.when(i == 4)
        def _():
            send(qg.at[c], qg.at[c], out_sem.at[4], q_sib, sib)

    def make_queries():
        await_bytes(qg.at[0], q_sib)

        def rows(n, carry):
            x = qg[n // 2, pl.ds((n % 2) * 4, 4)].reshape(192, 384)
            p = lax.dot_general(x, wq[...], NT, preferred_element_type=F32)
            nope, rot = p[:, :128], p[:, 128:]
            total = jnp.sum(nope * nope + jnp.where(lane < 64, rot * rot, 0.0), axis=1, keepdims=True)
            scale = lax.rsqrt(total * (1.0 / 192.0) + EPSILON) * (SCORE * LOG2E)
            angles = turning(base_ref[pl.ds(n * 4, 4)].reshape(192, 128), turn_gain(gq))
            rot = jnp.where(lane < 64, turned(rot * angles), 0.0) * scale
            at = pl.ds(pl.multiple_of(n * 192, 192), 192)
            queries[at, 0:128] = (nope * gq[:, :128] * scale).astype(BF16)
            queries[at, 128:256] = rot.astype(BF16)
            acc[at] = jnp.zeros((192, 256), F32)
            return carry

        lax.fori_loop(0, 4, rows, 0)

    def attend(first, last):
        def keys_of(n, carry):
            rows = lg[pl.ds(n * 2, 2)].reshape(768, 384)
            kv = jnp.dot(rows[:, :256], wkv[...], preferred_element_type=F32)
            tail = rows[:, 256:].astype(F32)
            nope = kv[:, :128]
            total = jnp.sum(nope * nope + jnp.where(lane < 64, 0.0, tail), axis=1, keepdims=True)
            scale = lax.rsqrt(total * (1.0 / 192.0) + EPSILON)
            keys = jnp.concatenate(
                [nope * (kg[:, :128] * scale), jnp.where(lane < 64, tail, 0.0) * scale], axis=1
            ).astype(BF16)
            values = jnp.concatenate([kv[:, 128:].astype(BF16), jnp.ones((768, 128), BF16)], axis=1)
            for m in range(3):
                at = pl.ds(m * 256, 256)
                scores = lax.dot_general(queries[at], keys, NT, preferred_element_type=F32)
                acc[at] += jnp.dot(jnp.exp2(scores).astype(BF16), values, preferred_element_type=F32)
            return carry

        lax.fori_loop(first, last, keys_of, 0)

    def xblock(zo, h, core):
        return xg.at[(zo * 2 + h) * 2 + core]

    def xsend(ref, sem, device):
        send(ref, ref, out_sem.at[5], sem, device)

    def settle(g):
        await_bytes(outgoing.at[pl.ds(0, 7 + g)], a2a.at[g])
        row = lax.broadcasted_iota(jnp.int32, (HALF, HALF), 0)
        col = lax.broadcasted_iota(jnp.int32, (HALF, HALF), 1)
        moved = (row == (col % 8 // 4) * 32 + col // 8 * 4 + col % 4).astype(BF16)
        came = arrived[g * 8 : g * 8 + 8].astype(F32)
        own = xblock(z, g, c)
        for n in range(2):
            piece = came[:, n * 8 : n * 8 + 8].reshape(HALF, 1024).astype(BF16)
            own[:, n * 1024 : n * 1024 + 1024] = jnp.dot(moved, piece, preferred_element_type=F32).astype(BF16)
        xsend(own, xr.at[g], right)
        xsend(own, xl.at[g], left)
        xsend(own, xs_own.at[g], sib)

    def relay_rows(j):
        k, hr = j // 2 + 1, j % 2
        hl = hr + j // 6
        from_left, from_right = xblock((z - k + 8) % 8, hr, c), xblock((z + k) % 8, hl, c)
        await_bytes(from_left, xr.at[j])

        @pl.when(j <= 4)
        def _():
            xsend(from_left, xr.at[j + 2], right)

        xsend(from_left, xs_r.at[j], sib)
        await_bytes(from_right, xl.at[j])

        @pl.when(j <= 3)
        def _():
            xsend(from_right, xl.at[j + 2], left)

        @pl.when(j == 5)
        def _():
            xsend(from_right, xl.at[6], left)

        xsend(from_right, xs_l.at[j], sib)

    def expert_pair(i):
        j = i - 1
        started = (i + 7) // 8
        k = (j + 2) // 2
        g0 = started * ((j + 2) % 2)
        g1 = (1 - started) + started * (g0 + i // 7)
        n0 = ((z + started * (8 - k)) % 8) * 2 + g0
        n1 = ((z + started * k) % 8) * 2 + g1

        @pl.when(i == 0)
        def _():
            await_bytes(xg.at[0], xs_own.at[0])
            await_bytes(xg.at[0], xs_own.at[1])

        @pl.when(i > 0)
        def _():
            await_bytes(xg.at[0], xs_r.at[j])
            await_bytes(xg.at[0], xs_l.at[j])

        def one(h, carry):
            at = pl.ds(pl.multiple_of(h * 32, 32), 32)
            x = jnp.concatenate([xg[n0 * 2, at], xg[n0 * 2 + 1, at], xg[n1 * 2, at], xg[n1 * 2 + 1, at]], axis=0)
            gate = jnp.dot(x, wg[h], preferred_element_type=F32)
            up = jnp.dot(x, wu[h], preferred_element_type=F32)
            hidden = (gate / (1.0 + jnp.exp(-gate)) * up).astype(BF16)
            for n in range(4):
                cols = pl.ds(n * 512, 512)
                y = jnp.dot(hidden, wd[h, :, cols], preferred_element_type=F32).astype(BF16)
                pg[n0, at, cols] = y[0:32]
                pg[16 + n0, at, cols] = y[32:64]
                pg[n1, at, cols] = y[64:96]
                pg[16 + n1, at, cols] = y[96:128]
            return carry

        lax.fori_loop(0, 2, one, 0)
        send(pg.at[other * 16 + n0], sg.at[n0], out_sem.at[6], sgs.at[i * 2], sib)
        send(pg.at[other * 16 + n1], sg.at[n1], out_sem.at[6], sgs.at[i * 2 + 1], sib)

    def add_rows(out, terms, rows):
        def tile(n, carry):
            at = pl.ds(pl.multiple_of(n * 16, 16), 16)
            total = terms[0][at].astype(F32)
            for term in terms[1:]:
                total += term[at].astype(F32)
            out[at] = total.astype(BF16)
            return carry

        lax.fori_loop(0, rows // 16, tile, 0)

    def sums_event(m, first, last):
        k = 4 - (m + 1) // 2
        for side in range(2):
            h = m % 2 if side == 0 else 1 - m % 2
            zo = (z + k) % 8 if side == 0 else (z + 8 - k) % 8
            step = 2 * (k - 1) + h + 1 if k < 4 else 7
            which = (1 - side) if k < 4 else side
            await_bytes(sg.at[zo * 2 + h], sgs.at[step * 2 + which])
            mine_, recv, sems, device = (pg.at[c * 16 + zo * 2 + h], (rr, rl)[side], (rrs, rls)[side], (right, left)[side])
            terms = [mine_, sg.at[zo * 2 + h]]
            if m >= 2:
                await_bytes(recv.at[m - 2], sems.at[m - 2])
                terms.append(recv.at[m - 2])
            add_rows(mine_, terms, HALF)
            send(mine_, recv.at[m], out_sem.at[7], sems.at[m], device)
            if last > first:
                middle = (first + last) // 2
                attend(*((first, middle), (middle, last))[side])

    def sums_final():
        for h in range(2):
            await_bytes(sg.at[z * 2 + h], sgs.at[h])
            await_bytes(rr.at[6 - h], rrs.at[6 - h])
            await_bytes(rl.at[5 + h], rls.at[5 + h])
            own = pg.at[c * 16 + z * 2 + h]
            add_rows(own, [own, sg.at[z * 2 + h], rr.at[6 - h], rl.at[5 + h]], HALF)
        row = lax.broadcasted_iota(jnp.int32, (HALF, HALF), 0)
        col = lax.broadcasted_iota(jnp.int32, (HALF, HALF), 1)
        back = (col == (row % 8 // 4) * 32 + row // 8 * 4 + row % 4).astype(BF16)
        for g in range(2):
            rows = jnp.dot(back, pg[c * 16 + z * 2 + g], preferred_element_type=F32).reshape(8, 8, 2048)
            arrived[g * 8 : g * 8 + 8] = jnp.concatenate([rows[:, :, :1024], rows[:, :, 1024:]], axis=1).astype(BF16)
        for n in range(1, 16):
            send(arrived.at[n], returned.at[n], out_sem.at[8], ret, (back_from(n), t))
        returned[0] = arrived[0]

    def project():
        def piece(n, carry):
            core, quarter = n // 4, n % 4
            at = pl.ds(pl.multiple_of(core * 384, 384), 384)
            block_ = acc[at]
            heads = (block_[:, :128] / block_[:, 128:]).astype(BF16)
            y = jnp.dot(
                heads, wmix[:, pl.ds(pl.multiple_of(quarter * 512, 512), 512)], preferred_element_type=F32
            ).astype(BF16)
            for zo in range(8):
                mp[core * 16 + zo * 2 + quarter // 2, :, pl.ds(pl.multiple_of(quarter % 2 * 512, 512), 512)] = y[
                    zo * 48 : zo * 48 + 48
                ]
            return carry

        lax.fori_loop(0, 8, piece, 0)
        send(mp.at[pl.ds(other * 16, 16)], msg, out_sem.at[9], ms, sib)

    def mix_event(m):
        k = 4 - (m + 1) // 2
        if m == 0:
            await_bytes(msg, ms)
        for side in range(2):
            h = m % 2 if side == 0 else 1 - m % 2
            zo = (z + k) % 8 if side == 0 else (z + 8 - k) % 8
            mine_, recv, sems, device = (mp.at[c * 16 + zo * 2 + h], (mr, ml)[side], (mrs, mls)[side], (right, left)[side])
            terms = [mine_, msg.at[zo * 2 + h]]
            if m >= 2:
                await_bytes(recv.at[m - 2], sems.at[m - 2])
                terms.append(recv.at[m - 2])
            add_rows(mine_, terms, 48)
            send(mine_, recv.at[m], out_sem.at[10], sems.at[m], device)

    def mix_final():
        for h in range(2):
            await_bytes(mr.at[6 - h], mrs.at[6 - h])
            await_bytes(ml.at[5 + h], mls.at[5 + h])
            add_rows(
                mix_ref.at[:, pl.ds(h * 1024, 1024)],
                [mp.at[c * 16 + z * 2 + h], msg.at[z * 2 + h], mr.at[6 - h], ml.at[5 + h]],
                48,
            )

    def combine():
        await_bytes(outgoing.at[pl.ds(0, 15)], ret)
        came = returned[...].astype(F32)
        for n in range(2):
            piece = came[:, n * 8 : n * 8 + 8].reshape(128, 1024).astype(BF16)
            total = jnp.zeros((48, 1024), F32)
            for k in range(2):
                total += jnp.dot(st[k], piece, preferred_element_type=F32) * column(route_ref[k : k + 1])
            expert_ref[:, n * 1024 : n * 1024 + 1024] = total.astype(BF16)

    relay_queries(0)
    settle(0)
    settle(1)
    start_latents()
    for load in loads[12:]:
        load.wait()
    wq[0:192] = wq_ref[...]
    wq[192:224] = wq_ref[160:192]
    wq[224:256] = wq_ref[128:160]
    wkv[:, 0:128] = wk_ref[...]
    wkv[:, 128:256] = wv_ref[...]

    def step(i, carry):
        @pl.when(i == 1)
        def _():
            relay_a()

        @pl.when(i == 2)
        def _():
            relay_a_far()
            relay_b(0)

        @pl.when(i == 3)
        def _():
            relay_b_far(0)
            relay_b(1)

        @pl.when(i == 4)
        def _():
            relay_b_far(2)
            relay_b(3)

        @pl.when(i == 5)
        def _():
            relay_b_far(3)
            make_queries()
            await_bytes(lg.at[pl.ds(0, 16)], ls)

        @pl.when((i >= 1) & (i <= 4))
        def _():
            relay_queries(i)

        expert_pair(i)

        @pl.when(i == 3)
        def _():
            relay_b_far(1)
            relay_b(2)

        @pl.when(i >= 5)
        def _():
            attend((i - 5) * 2, (i - 4) * 2)

        relay_rows(i)
        return carry

    lax.fori_loop(0, 7, step, 0)
    expert_pair(7)
    sums_event(0, 0, 0)
    sums_event(1, 0, 0)
    for m in range(2, 7):
        sums_event(m, 4 + (m - 2) * 12 // 5, 4 + (m - 1) * 12 // 5)
    project()
    mix_event(0)
    mix_event(1)
    sums_final()
    for m in range(2, 7):
        mix_event(m)
    combine()
    mix_final()

    await_bytes(outgoing.at[pl.ds(0, 15)], out_sem.at[0])
    await_bytes(lg.at[0, pl.ds(0, 7)], out_sem.at[1])
    await_bytes(qg.at[0, pl.ds(0, 7)], out_sem.at[2])
    await_bytes(lg.at[pl.ds(0, 31)], out_sem.at[3])
    await_bytes(qg.at[0], out_sem.at[4])
    await_bytes(xg.at[pl.ds(0, 30)], out_sem.at[5])
    await_bytes(xg.at[pl.ds(0, 16)], out_sem.at[6])
    await_bytes(xg.at[pl.ds(0, 14)], out_sem.at[7])
    await_bytes(outgoing.at[pl.ds(0, 15)], out_sem.at[8])
    await_bytes(msg, out_sem.at[9])
    await_bytes(mp.at[pl.ds(0, 14)], out_sem.at[10])


def on_device(
    q_latent, kv_latent, rope_key, q_latent_gain, kv_latent_gain, w_query, w_key, w_value, query_gain, key_gain,
    w_mix, tokens_b, norm_gain, expert_ids, route_weights, w_gate, w_up, w_down,
):
    base, shift = rope_tables()
    operands = (
        tokens_b, norm_gain, expert_ids.T, q_latent, kv_latent, rope_key, q_latent_gain, kv_latent_gain, query_gain,
        key_gain, jnp.asarray(base), jnp.asarray(shift), w_query.T, w_key, w_value, route_weights.T, w_gate, w_up, w_down,
        w_mix,
    )
    vmem = pl.BlockSpec(memory_space=pltpu.VMEM)
    hbm = pl.BlockSpec(memory_space=pl.ANY)
    dma = pltpu.SemaphoreType.DMA
    out = jax.ShapeDtypeStruct((48, 2048), BF16)
    results = pl.pallas_call(
        layer,
        out_shape=(out, out),
        in_specs=[hbm] * 20,
        out_specs=(vmem, vmem),
        scratch_shapes=[
            *[pltpu.VMEM(a.shape, a.dtype) for a in operands],
            pltpu.VMEM((256, 384), BF16),
            pltpu.VMEM((256, 256), BF16),
            pltpu.VMEM((2, 8, 48, 384), BF16),
            pltpu.VMEM((768, 256), BF16),
            pltpu.VMEM((768, 256), F32),
            pltpu.VMEM((32, 8, 48, 384), BF16),
            pltpu.VMEM((2, 48, 128), BF16),
            pltpu.VMEM((16, 16, 1024), BF16),
            pltpu.VMEM((16, 16, 1024), BF16),
            pltpu.VMEM((16, 16, 1024), BF16),
            pltpu.VMEM((32, HALF, 2048), BF16),
            pltpu.VMEM((32, HALF, 2048), BF16),
            pltpu.VMEM((16, HALF, 2048), BF16),
            pltpu.VMEM((7, HALF, 2048), BF16),
            pltpu.VMEM((7, HALF, 2048), BF16),
            pltpu.VMEM((32, 48, 1024), BF16),
            pltpu.VMEM((16, 48, 1024), BF16),
            pltpu.VMEM((7, 48, 1024), BF16),
            pltpu.VMEM((7, 48, 1024), BF16),
            dma((20,)),
            dma,
            dma((4,)),
            dma((3,)),
            dma,
            dma((4,)),
            dma((4, 4)),
            dma,
            dma((2,)),
            dma,
            dma((7,)),
            dma((7,)),
            dma((2,)),
            dma((7,)),
            dma((7,)),
            dma((16,)),
            dma((7,)),
            dma((7,)),
            dma,
            dma((7,)),
            dma((7,)),
            dma((11,)),
        ],
        compiler_params=pltpu.CompilerParams(
            collective_id=0, has_side_effects=True, vmem_limit_bytes=67_043_328
        ),
    )(*operands)
    return pl.pallas_call(hand_over, out_shape=(out, out), in_specs=[vmem] * 2, out_specs=(vmem, vmem))(*results)


def hand_over(mix_ref, expert_ref, mix_out, expert_out):
    mix_out[...] = mix_ref[...]
    expert_out[...] = expert_ref[...]


def solution(mesh):
    rows, whole = P(("ep", "tp"), None), P()
    in_specs = (
        rows, rows, rows, whole, whole, P(None, "tp"), P(None, "tp"), P(None, "tp"), whole, whole, P("tp", None), rows,
        whole, rows, rows, P("ep", None, "tp"), P("ep", None, "tp"), P("ep", "tp", None),
    )
    return jax.shard_map(on_device, mesh=mesh, in_specs=in_specs, out_specs=(rows, rows), check_vma=False)
```

```python
import jax
import jax.numpy as jnp
import numpy as np
from jax import lax
from jax.experimental import pallas as pl
from jax.experimental.pallas import tpu as pltpu
from jax.sharding import PartitionSpec as P

F32, BF16 = jnp.float32, jnp.bfloat16
MESH = pl.DeviceIdType.MESH
EPSILON = 1e-06
THETA = 10000.0
LOG2E = 1.4426950408889634
SCORE = 192 ** (-0.5)
NT = (((1,), (1,)), ((), ()))
TN = (((0,), (0,)), ((), ()))
HALF = 64
OFFSETS = (
    (0, 0), (0, 1), (1, 0), (0, 3), (3, 0), (1, 1), (3, 3), (0, 2), (2, 0), (1, 3), (3, 1), (2, 1), (1, 2), (2, 3), (3, 2), (2, 2),
)


def rope_tables():
    inverse = THETA ** (-np.arange(0, 64, 2, dtype=np.float64) / 64)
    rows = np.arange(768).reshape(8, 2, 48).transpose(1, 0, 2).reshape(768)
    angle = np.tile(rows[:, None] * inverse[None, :], (1, 2))
    base = np.concatenate([np.cos(angle), np.sin(angle)], axis=1).astype(np.float32)
    offset = np.tile((np.arange(16) * 768)[:, None] * inverse[None, :], (1, 4))
    shift = np.stack([np.cos(offset), np.sin(offset)], axis=1).astype(np.float32)
    return base.reshape(16, 48, 128), shift.reshape(16, 2, 128)


def send(src, dst, send_sem, recv_sem, device):
    pltpu.make_async_remote_copy(
        src_ref=src, dst_ref=dst, send_sem=send_sem, recv_sem=recv_sem, device_id=device, device_id_type=MESH
    ).start()


def await_bytes(ref, sem):
    pltpu.make_async_copy(ref, ref, sem).wait()


def normed(x, gain):
    return x * lax.rsqrt(jnp.mean(x * x, axis=-1, keepdims=True) + EPSILON) * gain


def layer(
    *refs,
):
    inputs, (mix_ref, expert_ref), held = refs[:20], refs[20:22], refs[22:42]
    (
        tokens_ref, b_gain, ids_ref, ql_ref, kvl_ref, rope_ref, ql_gain, kvl_gain, q_gain, k_gain, base_ref, shift_ref,
        wq_ref, wk_ref, wv_ref, route_ref, wg, wu, wd, wmix,
    ) = held
    (
    wq, wkv, qg, queries, acc, lg, st, outgoing, arrived, returned, xg, pg, sg, rr, rl, mp, msg, mr, ml,
    w_sem, z_sem, qr, ql, q_sib, la, lb, ls, a2a, ret, xr, xl, xs_own, xs_r, xs_l, sgs, rrs, rls, ms, mrs, mls, out_sem,
    ) = refs[42:]
    e, t = lax.axis_index("ep"), lax.axis_index("tp")
    z, c = t // 2, t % 2
    other = 1 - c
    sib = (e, z * 2 + other)

    def zpeer(d):
        return (e, ((z + d) % 8) * 2 + c)

    right, left = zpeer(1), zpeer(7)
    ey, ex = e // 4, e % 4
    pa = other * ex + c * ey
    pb = other * ey + c * ex

    def away(n):
        dy, dx = OFFSETS[n]
        return ((ey + dy) % 4) * 4 + (ex + dx) % 4

    def back_from(n):
        dy, dx = OFFSETS[n]
        return ((ey + 4 - dy) % 4) * 4 + (ex + 4 - dx) % 4

    def origin(da, db):
        a, b = (pa + da + 4) % 4, (pb + db + 4) % 4
        return other * (b * 4 + a) + c * (a * 4 + b)

    barrier = pltpu.get_barrier_semaphore()
    for d in range(1, 8):
        pl.semaphore_signal(barrier, inc=1, device_id=zpeer(d), device_id_type=MESH)
    for d in range(1, 16):
        pl.semaphore_signal(barrier, inc=1, device_id=((e + d) % 16, t), device_id_type=MESH)
    pl.semaphore_signal(barrier, inc=1, device_id=sib, device_id_type=MESH)

    loads = [pltpu.make_async_copy(src, dst, w_sem.at[n]) for n, (src, dst) in enumerate(zip(inputs, held))]
    for load in loads[:12]:
        load.start()
    for load in loads[:3]:
        load.wait()

    row48 = lax.broadcasted_iota(jnp.int32, (48, 48), 0)
    col48 = lax.broadcasted_iota(jnp.int32, (48, 48), 1)

    def column(x):
        return jnp.sum(jnp.where(row48 == col48, x, 0.0), axis=1, keepdims=True)

    ids = [column(ids_ref[k : k + 1].astype(F32)) for k in range(2)]
    place32 = lax.broadcasted_iota(jnp.int32, (1, 32), 1)
    experts = place32 % 2 * 1.0
    for n in range(16):
        experts += jnp.where(place32 // 2 == n, (away(n) * 2).astype(F32), 0.0)
    first_slot = (place32 * 4).astype(F32)
    hot = [(ids[k] == experts).astype(F32) for k in range(2)]
    lower = (row48 > col48).astype(BF16)
    before = [jnp.dot(lower, h.astype(BF16), preferred_element_type=F32) for h in hot]
    before[1] = before[1] + jnp.sum(hot[0], axis=0, keepdims=True)
    places = lax.broadcasted_iota(jnp.int32, (48, 128), 1).astype(F32)
    for k in range(2):
        rank = jnp.sum(hot[k] * before[k], axis=1, keepdims=True)
        slot = jnp.sum(hot[k] * first_slot, axis=1, keepdims=True) + rank
        st[k] = (slot == places).astype(BF16)
    b_normed = normed(tokens_ref[...].astype(F32), b_gain[...].reshape(1, 2048)).astype(BF16)
    slots = lax.dot_general(st[0] + st[1], b_normed, TN, preferred_element_type=F32)
    slots = slots.reshape(16, 8, 2048)
    outgoing[...] = jnp.concatenate([slots[:, :, :1024], slots[:, :, 1024:]], axis=1).astype(BF16)

    for load in loads[12:]:
        load.start()
    for load in loads[3:12]:
        load.wait()

    trig_q = shift_ref[pl.ds(e, 1), 0], shift_ref[pl.ds(e, 1), 1]
    lane = lax.broadcasted_iota(jnp.int32, (1, 128), 1)
    flip = jnp.where(lane < 64, -1.0, 1.0)

    def turning(u, gains):
        return (trig_q[0] * u + trig_q[1] * (pltpu.roll(u, 64, axis=1) * flip)) * gains

    def swapped(v):
        return jnp.concatenate([v, v[:, 32:64], v[:, 0:32]], axis=1)

    def turn_gain(g):
        tail = g[:, 128:192]
        return swapped(tail) * jnp.where((lane >= 64) & (lane < 96), -1.0, 1.0)

    gq, kg = q_gain[...].reshape(1, 192), k_gain[...].reshape(1, 192)

    def turned(v):
        return v + pltpu.roll(v, 64, axis=1)

    qg[c, z] = normed(ql_ref[...].astype(F32), ql_gain[...].reshape(1, 384)).astype(BF16)
    mine = lg.at[e * 2 + c, z]
    mine[:, 0:256] = normed(kvl_ref[...].astype(F32), kvl_gain[...].reshape(1, 256)).astype(BF16)
    rope = swapped(rope_ref[...].astype(F32))
    rope_rot = turned(rope * turning(base_ref[c * 8 + z], turn_gain(kg)))
    squares = jnp.sum(jnp.where(lane < 64, rope * rope, 0.0), axis=1, keepdims=True)
    high = squares.astype(BF16).astype(F32)
    mine[:, 256:384] = jnp.where(
        lane < 64, rope_rot, jnp.where(lane == 64, high, jnp.where(lane == 65, squares - high, 0.0))
    ).astype(BF16)

    pl.semaphore_wait(barrier, 23)
    for n in range(1, 16):
        send(outgoing.at[n], arrived.at[n], out_sem.at[0], a2a.at[n // 8], (away(n), t))
    for d in range(1, 8):
        send(mine, mine, out_sem.at[1], z_sem, zpeer(d))
    arrived[0] = outgoing[0]

    a_up, a_down = (origin(1, 0), t), (origin(-1, 0), t)
    b_up, b_down = (origin(0, 1), t), (origin(0, -1), t)

    def block(da, db):
        return lg.at[origin(da, db) * 2 + c]

    def part(da, db, n):
        return lg.at[origin(da, db) * 2 + c, pl.ds(4 * n, 4)]

    def full(ref, sem, device):
        send(ref, ref, out_sem.at[3], sem, device)

    def along_b(n, da):
        full(block(da, 0), lb.at[n, 0], b_up)
        full(block(da, 0), lb.at[n, 1], b_down)
        full(block(da, 0), ls, sib)

    def start_latents():
        await_bytes(lg.at[0, pl.ds(0, 7)], z_sem)
        full(block(0, 0), la.at[0], a_up)
        full(block(0, 0), la.at[1], a_down)
        along_b(0, 0)

    def relay_a():
        await_bytes(block(-1, 0), la.at[0])
        full(part(-1, 0, 0), la.at[2], a_up)
        along_b(1, -1)
        await_bytes(block(1, 0), la.at[1])
        full(part(1, 0, 1), la.at[3], a_down)
        along_b(2, 1)

    def relay_a_far():
        await_bytes(part(2, 0, 0), la.at[2])
        await_bytes(part(2, 0, 1), la.at[3])
        along_b(3, 2)

    def relay_b(n):
        da = (0, -1, 1, 2)[n]
        await_bytes(block(da, -1), lb.at[n, 0])
        full(part(da, -1, 0), lb.at[n, 2], b_up)
        full(block(da, -1), ls, sib)
        await_bytes(block(da, 1), lb.at[n, 1])
        full(part(da, 1, 1), lb.at[n, 3], b_down)
        full(block(da, 1), ls, sib)

    def relay_b_far(n):
        da = (0, -1, 1, 2)[n]
        await_bytes(part(da, 2, 0), lb.at[n, 2])
        await_bytes(part(da, 2, 1), lb.at[n, 3])
        full(block(da, 2), ls, sib)

    def relay_queries(i):
        from_left, from_right = qg.at[c, (z + 8 - i) % 8], qg.at[c, (z + i) % 8]

        @pl.when((i >= 1) & (i <= 4))
        def _():
            await_bytes(from_left, qr.at[i - 1])

        @pl.when((i >= 1) & (i <= 3))
        def _():
            await_bytes(from_right, ql.at[i - 1])

        @pl.when(i <= 3)
        def _():
            send(from_left, from_left, out_sem.at[2], qr.at[i], right)

        @pl.when(i <= 2)
        def _():
            send(from_right, from_right, out_sem.at[2], ql.at[i], left)

        @pl.when(i == 4)
        def _():
            send(qg.at[c], qg.at[c], out_sem.at[4], q_sib, sib)

    def make_queries():
        await_bytes(qg.at[0], q_sib)

        def rows(n, carry):
            x = qg[n // 2, pl.ds((n % 2) * 4, 4)].reshape(192, 384)
            p = lax.dot_general(x, wq[...], NT, preferred_element_type=F32)
            nope, rot = p[:, :128], p[:, 128:]
            total = jnp.sum(nope * nope + jnp.where(lane < 64, rot * rot, 0.0), axis=1, keepdims=True)
            scale = lax.rsqrt(total * (1.0 / 192.0) + EPSILON) * (SCORE * LOG2E)
            angles = turning(base_ref[pl.ds(n * 4, 4)].reshape(192, 128), turn_gain(gq))
            rot = jnp.where(lane < 64, turned(rot * angles), 0.0) * scale
            at = pl.ds(pl.multiple_of(n * 192, 192), 192)
            queries[at, 0:128] = (nope * gq[:, :128] * scale).astype(BF16)
            queries[at, 128:256] = rot.astype(BF16)
            acc[at] = jnp.zeros((192, 256), F32)
            return carry

        lax.fori_loop(0, 4, rows, 0)

    def attend(first, last):
        def keys_of(n, carry):
            rows = lg[pl.ds(n * 2, 2)].reshape(768, 384)
            kv = jnp.dot(rows[:, :256], wkv[...], preferred_element_type=F32)
            tail = rows[:, 256:].astype(F32)
            nope = kv[:, :128]
            total = jnp.sum(nope * nope + jnp.where(lane < 64, 0.0, tail), axis=1, keepdims=True)
            scale = lax.rsqrt(total * (1.0 / 192.0) + EPSILON)
            keys = jnp.concatenate(
                [nope * (kg[:, :128] * scale), jnp.where(lane < 64, tail, 0.0) * scale], axis=1
            ).astype(BF16)
            values = jnp.concatenate([kv[:, 128:].astype(BF16), jnp.ones((768, 128), BF16)], axis=1)
            for m in range(3):
                at = pl.ds(m * 256, 256)
                scores = lax.dot_general(queries[at], keys, NT, preferred_element_type=F32)
                acc[at] += jnp.dot(jnp.exp2(scores).astype(BF16), values, preferred_element_type=F32)
            return carry

        lax.fori_loop(first, last, keys_of, 0)

    def xblock(zo, h, core):
        return xg.at[(zo * 2 + h) * 2 + core]

    def xsend(ref, sem, device):
        send(ref, ref, out_sem.at[5], sem, device)

    def settle(g):
        await_bytes(outgoing.at[pl.ds(0, 7 + g)], a2a.at[g])
        row = lax.broadcasted_iota(jnp.int32, (HALF, HALF), 0)
        col = lax.broadcasted_iota(jnp.int32, (HALF, HALF), 1)
        moved = (row == (col % 8 // 4) * 32 + col // 8 * 4 + col % 4).astype(BF16)
        came = arrived[g * 8 : g * 8 + 8].astype(F32)
        own = xblock(z, g, c)
        for n in range(2):
            piece = came[:, n * 8 : n * 8 + 8].reshape(HALF, 1024).astype(BF16)
            own[:, n * 1024 : n * 1024 + 1024] = jnp.dot(moved, piece, preferred_element_type=F32).astype(BF16)
        xsend(own, xr.at[g], right)
        xsend(own, xl.at[g], left)
        xsend(own, xs_own.at[g], sib)

    def relay_rows(j):
        k, hr = j // 2 + 1, j % 2
        hl = hr + j // 6
        from_left, from_right = xblock((z - k + 8) % 8, hr, c), xblock((z + k) % 8, hl, c)
        await_bytes(from_left, xr.at[j])

        @pl.when(j <= 4)
        def _():
            xsend(from_left, xr.at[j + 2], right)

        xsend(from_left, xs_r.at[j], sib)
        await_bytes(from_right, xl.at[j])

        @pl.when(j <= 3)
        def _():
            xsend(from_right, xl.at[j + 2], left)

        @pl.when(j == 5)
        def _():
            xsend(from_right, xl.at[6], left)

        xsend(from_right, xs_l.at[j], sib)

    def expert_pair(i):
        j = i - 1
        started = (i + 7) // 8
        k = (j + 2) // 2
        g0 = started * ((j + 2) % 2)
        g1 = (1 - started) + started * (g0 + i // 7)
        n0 = ((z + started * (8 - k)) % 8) * 2 + g0
        n1 = ((z + started * k) % 8) * 2 + g1

        @pl.when(i == 0)
        def _():
            await_bytes(xg.at[0], xs_own.at[0])
            await_bytes(xg.at[0], xs_own.at[1])

        @pl.when(i > 0)
        def _():
            await_bytes(xg.at[0], xs_r.at[j])
            await_bytes(xg.at[0], xs_l.at[j])

        def one(h, carry):
            at = pl.ds(pl.multiple_of(h * 32, 32), 32)
            x = jnp.concatenate([xg[n0 * 2, at], xg[n0 * 2 + 1, at], xg[n1 * 2, at], xg[n1 * 2 + 1, at]], axis=0)
            gate = jnp.dot(x, wg[h], preferred_element_type=F32)
            up = jnp.dot(x, wu[h], preferred_element_type=F32)
            hidden = (gate / (1.0 + jnp.exp(-gate)) * up).astype(BF16)
            for n in range(4):
                cols = pl.ds(n * 512, 512)
                y = jnp.dot(hidden, wd[h, :, cols], preferred_element_type=F32).astype(BF16)
                pg[n0, at, cols] = y[0:32]
                pg[16 + n0, at, cols] = y[32:64]
                pg[n1, at, cols] = y[64:96]
                pg[16 + n1, at, cols] = y[96:128]
            return carry

        lax.fori_loop(0, 2, one, 0)
        send(pg.at[other * 16 + n0], sg.at[n0], out_sem.at[6], sgs.at[i * 2], sib)
        send(pg.at[other * 16 + n1], sg.at[n1], out_sem.at[6], sgs.at[i * 2 + 1], sib)

    def add_rows(out, terms, rows):
        def tile(n, carry):
            at = pl.ds(pl.multiple_of(n * 16, 16), 16)
            total = terms[0][at].astype(F32)
            for term in terms[1:]:
                total += term[at].astype(F32)
            out[at] = total.astype(BF16)
            return carry

        lax.fori_loop(0, rows // 16, tile, 0)

    def sums_event(m, first, last):
        k = 4 - (m + 1) // 2
        for side in range(2):
            h = m % 2 if side == 0 else 1 - m % 2
            zo = (z + k) % 8 if side == 0 else (z + 8 - k) % 8
            step = 2 * (k - 1) + h + 1 if k < 4 else 7
            which = (1 - side) if k < 4 else side
            await_bytes(sg.at[zo * 2 + h], sgs.at[step * 2 + which])
            mine_, recv, sems, device = (pg.at[c * 16 + zo * 2 + h], (rr, rl)[side], (rrs, rls)[side], (right, left)[side])
            terms = [mine_, sg.at[zo * 2 + h]]
            if m >= 2:
                await_bytes(recv.at[m - 2], sems.at[m - 2])
                terms.append(recv.at[m - 2])
            add_rows(mine_, terms, HALF)
            send(mine_, recv.at[m], out_sem.at[7], sems.at[m], device)
            if last > first:
                middle = (first + last) // 2
                attend(*((first, middle), (middle, last))[side])

    def sums_final():
        for h in range(2):
            await_bytes(sg.at[z * 2 + h], sgs.at[h])
            await_bytes(rr.at[6 - h], rrs.at[6 - h])
            await_bytes(rl.at[5 + h], rls.at[5 + h])
            own = pg.at[c * 16 + z * 2 + h]
            add_rows(own, [own, sg.at[z * 2 + h], rr.at[6 - h], rl.at[5 + h]], HALF)
        row = lax.broadcasted_iota(jnp.int32, (HALF, HALF), 0)
        col = lax.broadcasted_iota(jnp.int32, (HALF, HALF), 1)
        back = (col == (row % 8 // 4) * 32 + row // 8 * 4 + row % 4).astype(BF16)
        for g in range(2):
            rows = jnp.dot(back, pg[c * 16 + z * 2 + g], preferred_element_type=F32).reshape(8, 8, 2048)
            arrived[g * 8 : g * 8 + 8] = jnp.concatenate([rows[:, :, :1024], rows[:, :, 1024:]], axis=1).astype(BF16)
        for n in range(1, 16):
            send(arrived.at[n], returned.at[n], out_sem.at[8], ret, (back_from(n), t))
        returned[0] = arrived[0]

    def project():
        def piece(n, carry):
            core, quarter = n // 4, n % 4
            at = pl.ds(pl.multiple_of(core * 384, 384), 384)
            block_ = acc[at]
            heads = (block_[:, :128] / block_[:, 128:]).astype(BF16)
            y = jnp.dot(
                heads, wmix[:, pl.ds(pl.multiple_of(quarter * 512, 512), 512)], preferred_element_type=F32
            ).astype(BF16)
            for zo in range(8):
                mp[core * 16 + zo * 2 + quarter // 2, :, pl.ds(pl.multiple_of(quarter % 2 * 512, 512), 512)] = y[
                    zo * 48 : zo * 48 + 48
                ]
            return carry

        lax.fori_loop(0, 8, piece, 0)
        send(mp.at[pl.ds(other * 16, 16)], msg, out_sem.at[9], ms, sib)

    def mix_event(m):
        k = 4 - (m + 1) // 2
        if m == 0:
            await_bytes(msg, ms)
        for side in range(2):
            h = m % 2 if side == 0 else 1 - m % 2
            zo = (z + k) % 8 if side == 0 else (z + 8 - k) % 8
            mine_, recv, sems, device = (mp.at[c * 16 + zo * 2 + h], (mr, ml)[side], (mrs, mls)[side], (right, left)[side])
            terms = [mine_, msg.at[zo * 2 + h]]
            if m >= 2:
                await_bytes(recv.at[m - 2], sems.at[m - 2])
                terms.append(recv.at[m - 2])
            add_rows(mine_, terms, 48)
            send(mine_, recv.at[m], out_sem.at[10], sems.at[m], device)

    def mix_final():
        for h in range(2):
            await_bytes(mr.at[6 - h], mrs.at[6 - h])
            await_bytes(ml.at[5 + h], mls.at[5 + h])
            add_rows(
                mix_ref.at[:, pl.ds(h * 1024, 1024)],
                [mp.at[c * 16 + z * 2 + h], msg.at[z * 2 + h], mr.at[6 - h], ml.at[5 + h]],
                48,
            )

    def combine():
        await_bytes(outgoing.at[pl.ds(0, 15)], ret)
        came = returned[...].astype(F32)
        for n in range(2):
            piece = came[:, n * 8 : n * 8 + 8].reshape(128, 1024).astype(BF16)
            total = jnp.zeros((48, 1024), F32)
            for k in range(2):
                total += jnp.dot(st[k], piece, preferred_element_type=F32) * column(route_ref[k : k + 1])
            expert_ref[:, n * 1024 : n * 1024 + 1024] = total.astype(BF16)

    relay_queries(0)
    settle(0)
    start_latents()
    settle(1)
    for load in loads[12:]:
        load.wait()
    wq[0:192] = wq_ref[...]
    wq[192:224] = wq_ref[160:192]
    wq[224:256] = wq_ref[128:160]
    wkv[:, 0:128] = wk_ref[...]
    wkv[:, 128:256] = wv_ref[...]

    def step(i, carry):
        @pl.when(i == 1)
        def _():
            relay_a()
            relay_b(0)

        @pl.when(i == 2)
        def _():
            relay_a_far()

        @pl.when(i == 3)
        def _():
            relay_b(1)

        @pl.when(i == 4)
        def _():
            relay_b(2)

        @pl.when(i == 5)
        def _():
            relay_b(3)

        @pl.when((i >= 1) & (i <= 4))
        def _():
            relay_queries(i)

        expert_pair(i)

        @pl.when(i == 6)
        def _():
            make_queries()
            sums_event(1, 0, 0)

        relay_rows(i)
        return carry

    lax.fori_loop(0, 7, step, 0)
    expert_pair(7)
    sums_event(0, 0, 0)
    for n in range(4):
        relay_b_far(n)
    await_bytes(lg.at[pl.ds(0, 16)], ls)
    for n, m in enumerate((3, 2, 5, 4)):
        sums_event(m, n * 4, n * 4 + 4)
    project()
    sums_event(6, 0, 0)
    mix_event(0)
    mix_event(1)
    sums_final()
    for m in range(2, 7):
        mix_event(m)
    combine()
    mix_final()

    await_bytes(outgoing.at[pl.ds(0, 15)], out_sem.at[0])
    await_bytes(lg.at[0, pl.ds(0, 7)], out_sem.at[1])
    await_bytes(qg.at[0, pl.ds(0, 7)], out_sem.at[2])
    await_bytes(lg.at[pl.ds(0, 31)], out_sem.at[3])
    await_bytes(qg.at[0], out_sem.at[4])
    await_bytes(xg.at[pl.ds(0, 30)], out_sem.at[5])
    await_bytes(xg.at[pl.ds(0, 16)], out_sem.at[6])
    await_bytes(xg.at[pl.ds(0, 14)], out_sem.at[7])
    await_bytes(outgoing.at[pl.ds(0, 15)], out_sem.at[8])
    await_bytes(msg, out_sem.at[9])
    await_bytes(mp.at[pl.ds(0, 14)], out_sem.at[10])


def on_device(
    q_latent, kv_latent, rope_key, q_latent_gain, kv_latent_gain, w_query, w_key, w_value, query_gain, key_gain,
    w_mix, tokens_b, norm_gain, expert_ids, route_weights, w_gate, w_up, w_down,
):
    base, shift = rope_tables()
    operands = (
        tokens_b, norm_gain, expert_ids.T, q_latent, kv_latent, rope_key, q_latent_gain, kv_latent_gain, query_gain,
        key_gain, jnp.asarray(base), jnp.asarray(shift), w_query.T, w_key, w_value, route_weights.T, w_gate, w_up, w_down,
        w_mix,
    )
    vmem = pl.BlockSpec(memory_space=pltpu.VMEM)
    hbm = pl.BlockSpec(memory_space=pl.ANY)
    dma = pltpu.SemaphoreType.DMA
    out = jax.ShapeDtypeStruct((48, 2048), BF16)
    results = pl.pallas_call(
        layer,
        out_shape=(out, out),
        in_specs=[hbm] * 20,
        out_specs=(vmem, vmem),
        scratch_shapes=[
            *[pltpu.VMEM(a.shape, a.dtype) for a in operands],
            pltpu.VMEM((256, 384), BF16),
            pltpu.VMEM((256, 256), BF16),
            pltpu.VMEM((2, 8, 48, 384), BF16),
            pltpu.VMEM((768, 256), BF16),
            pltpu.VMEM((768, 256), F32),
            pltpu.VMEM((32, 8, 48, 384), BF16),
            pltpu.VMEM((2, 48, 128), BF16),
            pltpu.VMEM((16, 16, 1024), BF16),
            pltpu.VMEM((16, 16, 1024), BF16),
            pltpu.VMEM((16, 16, 1024), BF16),
            pltpu.VMEM((32, HALF, 2048), BF16),
            pltpu.VMEM((32, HALF, 2048), BF16),
            pltpu.VMEM((16, HALF, 2048), BF16),
            pltpu.VMEM((7, HALF, 2048), BF16),
            pltpu.VMEM((7, HALF, 2048), BF16),
            pltpu.VMEM((32, 48, 1024), BF16),
            pltpu.VMEM((16, 48, 1024), BF16),
            pltpu.VMEM((7, 48, 1024), BF16),
            pltpu.VMEM((7, 48, 1024), BF16),
            dma((20,)),
            dma,
            dma((4,)),
            dma((3,)),
            dma,
            dma((4,)),
            dma((4, 4)),
            dma,
            dma((2,)),
            dma,
            dma((7,)),
            dma((7,)),
            dma((2,)),
            dma((7,)),
            dma((7,)),
            dma((16,)),
            dma((7,)),
            dma((7,)),
            dma,
            dma((7,)),
            dma((7,)),
            dma((11,)),
        ],
        compiler_params=pltpu.CompilerParams(
            collective_id=0, has_side_effects=True, vmem_limit_bytes=67_043_328
        ),
    )(*operands)
    return pl.pallas_call(hand_over, out_shape=(out, out), in_specs=[vmem] * 2, out_specs=(vmem, vmem))(*results)


def hand_over(mix_ref, expert_ref, mix_out, expert_out):
    mix_out[...] = mix_ref[...]
    expert_out[...] = expert_ref[...]


def solution(mesh):
    rows, whole = P(("ep", "tp"), None), P()
    in_specs = (
        rows, rows, rows, whole, whole, P(None, "tp"), P(None, "tp"), P(None, "tp"), whole, whole, P("tp", None), rows,
        whole, rows, rows, P("ep", None, "tp"), P("ep", None, "tp"), P("ep", "tp", None),
    )
    return jax.shard_map(on_device, mesh=mesh, in_specs=in_specs, out_specs=(rows, rows), check_vma=False)
```

```python
import jax
import jax.numpy as jnp
import numpy as np
from jax import lax
from jax.experimental import pallas as pl
from jax.experimental.pallas import tpu as pltpu
from jax.sharding import PartitionSpec as P

F32, BF16 = jnp.float32, jnp.bfloat16
MESH = pl.DeviceIdType.MESH
EPSILON = 1e-06
THETA = 10000.0
LOG2E = 1.4426950408889634
SCORE = 192 ** (-0.5)
NT = (((1,), (1,)), ((), ()))
TN = (((0,), (0,)), ((), ()))
HALF = 64
OFFSETS = (
    (0, 0), (0, 1), (1, 0), (0, 3), (3, 0), (1, 1), (3, 3), (0, 2), (2, 0), (1, 3), (3, 1), (2, 1), (1, 2), (2, 3), (3, 2), (2, 2),
)


def rope_tables():
    inverse = THETA ** (-np.arange(0, 64, 2, dtype=np.float64) / 64)
    rows = np.arange(768).reshape(8, 2, 48).transpose(1, 0, 2).reshape(768)
    angle = np.tile(rows[:, None] * inverse[None, :], (1, 2))
    base = np.concatenate([np.cos(angle), np.sin(angle)], axis=1).astype(np.float32)
    offset = np.tile((np.arange(16) * 768)[:, None] * inverse[None, :], (1, 4))
    shift = np.stack([np.cos(offset), np.sin(offset)], axis=1).astype(np.float32)
    return base.reshape(16, 48, 128), shift.reshape(16, 2, 128)


def send(src, dst, send_sem, recv_sem, device):
    pltpu.make_async_remote_copy(
        src_ref=src, dst_ref=dst, send_sem=send_sem, recv_sem=recv_sem, device_id=device, device_id_type=MESH
    ).start()


def await_bytes(ref, sem):
    pltpu.make_async_copy(ref, ref, sem).wait()


def normed(x, gain):
    return x * lax.rsqrt(jnp.mean(x * x, axis=-1, keepdims=True) + EPSILON) * gain


def layer(
    *refs,
):
    inputs, (mix_ref, expert_ref), held = refs[:20], refs[20:22], refs[22:42]
    (
        tokens_ref, b_gain, ids_ref, ql_ref, kvl_ref, rope_ref, ql_gain, kvl_gain, q_gain, k_gain, base_ref, shift_ref,
        wq_ref, wk_ref, wv_ref, route_ref, wg, wu, wd, wmix,
    ) = held
    (
    wq, wkv, qg, queries, acc, lg, st, outgoing, arrived, returned, xg, pg, sg, rr, rl, mp, msg, mr, ml,
    w_sem, z_sem, qr, ql, q_sib, la, lb, ls, a2a, ret, xr, xl, xs_own, xs_r, xs_l, sgs, rrs, rls, ms, mrs, mls, out_sem,
    ) = refs[42:]
    e, t = lax.axis_index("ep"), lax.axis_index("tp")
    z, c = t // 2, t % 2
    other = 1 - c
    sib = (e, z * 2 + other)

    def zpeer(d):
        return (e, ((z + d) % 8) * 2 + c)

    right, left = zpeer(1), zpeer(7)
    ey, ex = e // 4, e % 4
    pa = other * ex + c * ey
    pb = other * ey + c * ex

    def away(n):
        dy, dx = OFFSETS[n]
        return ((ey + dy) % 4) * 4 + (ex + dx) % 4

    def back_from(n):
        dy, dx = OFFSETS[n]
        return ((ey + 4 - dy) % 4) * 4 + (ex + 4 - dx) % 4

    def origin(da, db):
        a, b = (pa + da + 4) % 4, (pb + db + 4) % 4
        return other * (b * 4 + a) + c * (a * 4 + b)

    barrier = pltpu.get_barrier_semaphore()
    for d in range(1, 8):
        pl.semaphore_signal(barrier, inc=1, device_id=zpeer(d), device_id_type=MESH)
    for d in range(1, 16):
        pl.semaphore_signal(barrier, inc=1, device_id=((e + d) % 16, t), device_id_type=MESH)
    pl.semaphore_signal(barrier, inc=1, device_id=sib, device_id_type=MESH)

    loads = [pltpu.make_async_copy(src, dst, w_sem.at[n]) for n, (src, dst) in enumerate(zip(inputs, held))]
    for load in loads[:12]:
        load.start()
    for load in loads[:3]:
        load.wait()

    row48 = lax.broadcasted_iota(jnp.int32, (48, 48), 0)
    col48 = lax.broadcasted_iota(jnp.int32, (48, 48), 1)

    def column(x):
        return jnp.sum(jnp.where(row48 == col48, x, 0.0), axis=1, keepdims=True)

    ids = [column(ids_ref[k : k + 1].astype(F32)) for k in range(2)]
    place32 = lax.broadcasted_iota(jnp.int32, (1, 32), 1)
    experts = place32 % 2 * 1.0
    for n in range(16):
        experts += jnp.where(place32 // 2 == n, (away(n) * 2).astype(F32), 0.0)
    first_slot = (place32 * 4).astype(F32)
    hot = [(ids[k] == experts).astype(F32) for k in range(2)]
    lower = (row48 > col48).astype(BF16)
    before = [jnp.dot(lower, h.astype(BF16), preferred_element_type=F32) for h in hot]
    before[1] = before[1] + jnp.sum(hot[0], axis=0, keepdims=True)
    places = lax.broadcasted_iota(jnp.int32, (48, 128), 1).astype(F32)
    for k in range(2):
        rank = jnp.sum(hot[k] * before[k], axis=1, keepdims=True)
        slot = jnp.sum(hot[k] * first_slot, axis=1, keepdims=True) + rank
        st[k] = (slot == places).astype(BF16)
    b_normed = normed(tokens_ref[...].astype(F32), b_gain[...].reshape(1, 2048)).astype(BF16)
    slots = lax.dot_general(st[0] + st[1], b_normed, TN, preferred_element_type=F32)
    slots = slots.reshape(16, 8, 2048)
    outgoing[...] = jnp.concatenate([slots[:, :, :1024], slots[:, :, 1024:]], axis=1).astype(BF16)

    for load in loads[12:]:
        load.start()
    for load in loads[3:12]:
        load.wait()

    trig_q = shift_ref[pl.ds(e, 1), 0], shift_ref[pl.ds(e, 1), 1]
    lane = lax.broadcasted_iota(jnp.int32, (1, 128), 1)
    flip = jnp.where(lane < 64, -1.0, 1.0)

    def turning(u, gains):
        return (trig_q[0] * u + trig_q[1] * (pltpu.roll(u, 64, axis=1) * flip)) * gains

    def swapped(v):
        return jnp.concatenate([v, v[:, 32:64], v[:, 0:32]], axis=1)

    def turn_gain(g):
        tail = g[:, 128:192]
        return swapped(tail) * jnp.where((lane >= 64) & (lane < 96), -1.0, 1.0)

    gq, kg = q_gain[...].reshape(1, 192), k_gain[...].reshape(1, 192)

    def turned(v):
        return v + pltpu.roll(v, 64, axis=1)

    qg[c, z] = normed(ql_ref[...].astype(F32), ql_gain[...].reshape(1, 384)).astype(BF16)
    mine = lg.at[e * 2 + c, z]
    mine[:, 0:256] = normed(kvl_ref[...].astype(F32), kvl_gain[...].reshape(1, 256)).astype(BF16)
    rope = swapped(rope_ref[...].astype(F32))
    rope_rot = turned(rope * turning(base_ref[c * 8 + z], turn_gain(kg)))
    squares = jnp.sum(jnp.where(lane < 64, rope * rope, 0.0), axis=1, keepdims=True)
    high = squares.astype(BF16).astype(F32)
    mine[:, 256:384] = jnp.where(
        lane < 64, rope_rot, jnp.where(lane == 64, high, jnp.where(lane == 65, squares - high, 0.0))
    ).astype(BF16)

    pl.semaphore_wait(barrier, 23)
    for n in range(1, 16):
        send(outgoing.at[n], arrived.at[n], out_sem.at[0], a2a.at[n // 8], (away(n), t))
    for d in range(1, 8):
        send(mine, mine, out_sem.at[1], z_sem, zpeer(d))
    arrived[0] = outgoing[0]

    a_up, a_down = (origin(1, 0), t), (origin(-1, 0), t)
    b_up, b_down = (origin(0, 1), t), (origin(0, -1), t)

    def block(da, db):
        return lg.at[origin(da, db) * 2 + c]

    def part(da, db, n):
        return lg.at[origin(da, db) * 2 + c, pl.ds(4 * n, 4)]

    def full(ref, sem, device):
        send(ref, ref, out_sem.at[3], sem, device)

    def along_b(n, da):
        full(block(da, 0), lb.at[n, 0], b_up)
        full(block(da, 0), lb.at[n, 1], b_down)
        full(block(da, 0), ls, sib)

    def start_latents():
        await_bytes(lg.at[0, pl.ds(0, 7)], z_sem)
        full(block(0, 0), la.at[0], a_up)
        full(block(0, 0), la.at[1], a_down)
        along_b(0, 0)

    def relay_a():
        await_bytes(block(-1, 0), la.at[0])
        full(part(-1, 0, 0), la.at[2], a_up)
        along_b(1, -1)
        await_bytes(block(1, 0), la.at[1])
        full(part(1, 0, 1), la.at[3], a_down)
        along_b(2, 1)

    def relay_a_far():
        await_bytes(part(2, 0, 0), la.at[2])
        await_bytes(part(2, 0, 1), la.at[3])
        along_b(3, 2)

    def relay_b(n):
        da = (0, -1, 1, 2)[n]
        await_bytes(block(da, -1), lb.at[n, 0])
        full(part(da, -1, 0), lb.at[n, 2], b_up)
        full(block(da, -1), ls, sib)
        await_bytes(block(da, 1), lb.at[n, 1])
        full(part(da, 1, 1), lb.at[n, 3], b_down)
        full(block(da, 1), ls, sib)

    def relay_b_far(n):
        da = (0, -1, 1, 2)[n]
        await_bytes(part(da, 2, 0), lb.at[n, 2])
        await_bytes(part(da, 2, 1), lb.at[n, 3])
        full(block(da, 2), ls, sib)

    def relay_queries(i):
        from_left, from_right = qg.at[c, (z + 8 - i) % 8], qg.at[c, (z + i) % 8]

        @pl.when((i >= 1) & (i <= 4))
        def _():
            await_bytes(from_left, qr.at[i - 1])

        @pl.when((i >= 1) & (i <= 3))
        def _():
            await_bytes(from_right, ql.at[i - 1])

        @pl.when(i <= 3)
        def _():
            send(from_left, from_left, out_sem.at[2], qr.at[i], right)

        @pl.when(i <= 2)
        def _():
            send(from_right, from_right, out_sem.at[2], ql.at[i], left)

        @pl.when(i == 4)
        def _():
            send(qg.at[c], qg.at[c], out_sem.at[4], q_sib, sib)

    def make_queries():
        await_bytes(qg.at[0], q_sib)

        def rows(n, carry):
            x = qg[n // 2, pl.ds((n % 2) * 4, 4)].reshape(192, 384)
            p = lax.dot_general(x, wq[...], NT, preferred_element_type=F32)
            nope, rot = p[:, :128], p[:, 128:]
            total = jnp.sum(nope * nope + jnp.where(lane < 64, rot * rot, 0.0), axis=1, keepdims=True)
            scale = lax.rsqrt(total * (1.0 / 192.0) + EPSILON) * (SCORE * LOG2E)
            angles = turning(base_ref[pl.ds(n * 4, 4)].reshape(192, 128), turn_gain(gq))
            rot = jnp.where(lane < 64, turned(rot * angles), 0.0) * scale
            at = pl.ds(pl.multiple_of(n * 192, 192), 192)
            queries[at, 0:128] = (nope * gq[:, :128] * scale).astype(BF16)
            queries[at, 128:256] = rot.astype(BF16)
            acc[at] = jnp.zeros((192, 256), F32)
            return carry

        lax.fori_loop(0, 4, rows, 0)

    def attend(first, last):
        def keys_of(n, carry):
            rows = lg[pl.ds(n * 2, 2)].reshape(768, 384)
            kv = jnp.dot(rows[:, :256], wkv[...], preferred_element_type=F32)
            tail = rows[:, 256:].astype(F32)
            nope = kv[:, :128]
            total = jnp.sum(nope * nope + jnp.where(lane < 64, 0.0, tail), axis=1, keepdims=True)
            scale = lax.rsqrt(total * (1.0 / 192.0) + EPSILON)
            keys = jnp.concatenate(
                [nope * (kg[:, :128] * scale), jnp.where(lane < 64, tail, 0.0) * scale], axis=1
            ).astype(BF16)
            values = jnp.concatenate([kv[:, 128:].astype(BF16), jnp.ones((768, 128), BF16)], axis=1)
            for m in range(3):
                at = pl.ds(m * 256, 256)
                scores = lax.dot_general(queries[at], keys, NT, preferred_element_type=F32)
                acc[at] += jnp.dot(jnp.exp2(scores).astype(BF16), values, preferred_element_type=F32)
            return carry

        lax.fori_loop(first, last, keys_of, 0)

    def xblock(zo, h, core):
        return xg.at[(zo * 2 + h) * 2 + core]

    def xsend(ref, sem, device):
        send(ref, ref, out_sem.at[5], sem, device)

    def settle(g):
        await_bytes(outgoing.at[pl.ds(0, 7 + g)], a2a.at[g])
        row = lax.broadcasted_iota(jnp.int32, (HALF, HALF), 0)
        col = lax.broadcasted_iota(jnp.int32, (HALF, HALF), 1)
        moved = (row == (col % 8 // 4) * 32 + col // 8 * 4 + col % 4).astype(BF16)
        came = arrived[g * 8 : g * 8 + 8].astype(F32)
        own = xblock(z, g, c)
        for n in range(2):
            piece = came[:, n * 8 : n * 8 + 8].reshape(HALF, 1024).astype(BF16)
            own[:, n * 1024 : n * 1024 + 1024] = jnp.dot(moved, piece, preferred_element_type=F32).astype(BF16)
        xsend(own, xr.at[g], right)
        xsend(own, xl.at[g], left)
        xsend(own, xs_own.at[g], sib)

    def relay_rows(j):
        k, hr = j // 2 + 1, j % 2
        hl = hr + j // 6
        from_left, from_right = xblock((z - k + 8) % 8, hr, c), xblock((z + k) % 8, hl, c)
        await_bytes(from_left, xr.at[j])

        @pl.when(j <= 4)
        def _():
            xsend(from_left, xr.at[j + 2], right)

        xsend(from_left, xs_r.at[j], sib)
        await_bytes(from_right, xl.at[j])

        @pl.when(j <= 3)
        def _():
            xsend(from_right, xl.at[j + 2], left)

        @pl.when(j == 5)
        def _():
            xsend(from_right, xl.at[6], left)

        xsend(from_right, xs_l.at[j], sib)

    def expert_pair(i):
        j = i - 1
        started = (i + 7) // 8
        k = (j + 2) // 2
        g0 = started * ((j + 2) % 2)
        g1 = (1 - started) + started * (g0 + i // 7)
        n0 = ((z + started * (8 - k)) % 8) * 2 + g0
        n1 = ((z + started * k) % 8) * 2 + g1

        @pl.when(i == 0)
        def _():
            await_bytes(xg.at[0], xs_own.at[0])
            await_bytes(xg.at[0], xs_own.at[1])

        @pl.when(i > 0)
        def _():
            await_bytes(xg.at[0], xs_r.at[j])
            await_bytes(xg.at[0], xs_l.at[j])

        def one(h, carry):
            at = pl.ds(pl.multiple_of(h * 32, 32), 32)
            x = jnp.concatenate([xg[n0 * 2, at], xg[n0 * 2 + 1, at], xg[n1 * 2, at], xg[n1 * 2 + 1, at]], axis=0)
            gate = jnp.dot(x, wg[h], preferred_element_type=F32)
            up = jnp.dot(x, wu[h], preferred_element_type=F32)
            hidden = (gate / (1.0 + jnp.exp(-gate)) * up).astype(BF16)
            for n in range(4):
                cols = pl.ds(n * 512, 512)
                y = jnp.dot(hidden, wd[h, :, cols], preferred_element_type=F32).astype(BF16)
                pg[n0, at, cols] = y[0:32]
                pg[16 + n0, at, cols] = y[32:64]
                pg[n1, at, cols] = y[64:96]
                pg[16 + n1, at, cols] = y[96:128]
            return carry

        lax.fori_loop(0, 2, one, 0)
        send(pg.at[other * 16 + n0], sg.at[n0], out_sem.at[6], sgs.at[i * 2], sib)
        send(pg.at[other * 16 + n1], sg.at[n1], out_sem.at[6], sgs.at[i * 2 + 1], sib)

    def add_rows(out, terms, rows):
        def tile(n, carry):
            at = pl.ds(pl.multiple_of(n * 16, 16), 16)
            total = terms[0][at].astype(F32)
            for term in terms[1:]:
                total += term[at].astype(F32)
            out[at] = total.astype(BF16)
            return carry

        lax.fori_loop(0, rows // 16, tile, 0)

    def sums_event(m, first, last):
        k = 4 - (m + 1) // 2
        for side in range(2):
            h = m % 2 if side == 0 else 1 - m % 2
            zo = (z + k) % 8 if side == 0 else (z + 8 - k) % 8
            step = 2 * (k - 1) + h + 1 if k < 4 else 7
            which = (1 - side) if k < 4 else side
            await_bytes(sg.at[zo * 2 + h], sgs.at[step * 2 + which])
            mine_, recv, sems, device = (pg.at[c * 16 + zo * 2 + h], (rr, rl)[side], (rrs, rls)[side], (right, left)[side])
            terms = [mine_, sg.at[zo * 2 + h]]
            if m >= 2:
                await_bytes(recv.at[m - 2], sems.at[m - 2])
                terms.append(recv.at[m - 2])
            add_rows(mine_, terms, HALF)
            send(mine_, recv.at[m], out_sem.at[7], sems.at[m], device)
            if last > first:
                middle = (first + last) // 2
                attend(*((first, middle), (middle, last))[side])

    def sums_final():
        for h in range(2):
            await_bytes(sg.at[z * 2 + h], sgs.at[h])
            await_bytes(rr.at[6 - h], rrs.at[6 - h])
            await_bytes(rl.at[5 + h], rls.at[5 + h])
            own = pg.at[c * 16 + z * 2 + h]
            add_rows(own, [own, sg.at[z * 2 + h], rr.at[6 - h], rl.at[5 + h]], HALF)
        row = lax.broadcasted_iota(jnp.int32, (HALF, HALF), 0)
        col = lax.broadcasted_iota(jnp.int32, (HALF, HALF), 1)
        back = (col == (row % 8 // 4) * 32 + row // 8 * 4 + row % 4).astype(BF16)
        for g in range(2):
            rows = jnp.dot(back, pg[c * 16 + z * 2 + g], preferred_element_type=F32).reshape(8, 8, 2048)
            arrived[g * 8 : g * 8 + 8] = jnp.concatenate([rows[:, :, :1024], rows[:, :, 1024:]], axis=1).astype(BF16)
        for n in range(1, 16):
            send(arrived.at[n], returned.at[n], out_sem.at[8], ret, (back_from(n), t))
        returned[0] = arrived[0]

    def project():
        def piece(n, carry):
            core, quarter = n // 4, n % 4
            at = pl.ds(pl.multiple_of(core * 384, 384), 384)
            block_ = acc[at]
            heads = (block_[:, :128] / block_[:, 128:]).astype(BF16)
            y = jnp.dot(
                heads, wmix[:, pl.ds(pl.multiple_of(quarter * 512, 512), 512)], preferred_element_type=F32
            ).astype(BF16)
            for zo in range(8):
                mp[core * 16 + zo * 2 + quarter // 2, :, pl.ds(pl.multiple_of(quarter % 2 * 512, 512), 512)] = y[
                    zo * 48 : zo * 48 + 48
                ]
            return carry

        lax.fori_loop(0, 8, piece, 0)
        send(mp.at[pl.ds(other * 16, 16)], msg, out_sem.at[9], ms, sib)

    def mix_event(m):
        k = 4 - (m + 1) // 2
        if m == 0:
            await_bytes(msg, ms)
        for side in range(2):
            h = m % 2 if side == 0 else 1 - m % 2
            zo = (z + k) % 8 if side == 0 else (z + 8 - k) % 8
            mine_, recv, sems, device = (mp.at[c * 16 + zo * 2 + h], (mr, ml)[side], (mrs, mls)[side], (right, left)[side])
            terms = [mine_, msg.at[zo * 2 + h]]
            if m >= 2:
                await_bytes(recv.at[m - 2], sems.at[m - 2])
                terms.append(recv.at[m - 2])
            add_rows(mine_, terms, 48)
            send(mine_, recv.at[m], out_sem.at[10], sems.at[m], device)

    def mix_final():
        for h in range(2):
            await_bytes(mr.at[6 - h], mrs.at[6 - h])
            await_bytes(ml.at[5 + h], mls.at[5 + h])
            add_rows(
                mix_ref.at[:, pl.ds(h * 1024, 1024)],
                [mp.at[c * 16 + z * 2 + h], msg.at[z * 2 + h], mr.at[6 - h], ml.at[5 + h]],
                48,
            )

    def combine():
        await_bytes(outgoing.at[pl.ds(0, 15)], ret)
        came = returned[...].astype(F32)
        for n in range(2):
            piece = came[:, n * 8 : n * 8 + 8].reshape(128, 1024).astype(BF16)
            total = jnp.zeros((48, 1024), F32)
            for k in range(2):
                total += jnp.dot(st[k], piece, preferred_element_type=F32) * column(route_ref[k : k + 1])
            expert_ref[:, n * 1024 : n * 1024 + 1024] = total.astype(BF16)

    relay_queries(0)
    settle(0)
    start_latents()
    settle(1)
    for load in loads[12:]:
        load.wait()
    wq[0:192] = wq_ref[...]
    wq[192:224] = wq_ref[160:192]
    wq[224:256] = wq_ref[128:160]
    wkv[:, 0:128] = wk_ref[...]
    wkv[:, 128:256] = wv_ref[...]

    def step(i, carry):
        @pl.when(i == 1)
        def _():
            relay_a()
            relay_b(0)

        @pl.when(i == 2)
        def _():
            relay_a_far()

        @pl.when(i == 3)
        def _():
            relay_b(1)

        @pl.when(i == 4)
        def _():
            relay_b(2)

        @pl.when(i == 5)
        def _():
            relay_b(3)

        @pl.when((i >= 1) & (i <= 4))
        def _():
            relay_queries(i)

        expert_pair(i)

        @pl.when(i == 6)
        def _():
            make_queries()
            sums_event(1, 0, 0)

        relay_rows(i)
        return carry

    lax.fori_loop(0, 7, step, 0)
    expert_pair(7)
    sums_event(0, 0, 0)
    for n in range(4):
        relay_b_far(n)
    await_bytes(lg.at[pl.ds(0, 16)], ls)
    for n, m in enumerate((3, 2, 5, 4)):
        sums_event(m, n * 4, n * 4 + 4)
    project()
    mix_event(0)
    sums_event(6, 0, 0)
    mix_event(1)
    mix_event(2)
    sums_final()
    for m in range(3, 7):
        mix_event(m)
    combine()
    mix_final()

    await_bytes(outgoing.at[pl.ds(0, 15)], out_sem.at[0])
    await_bytes(lg.at[0, pl.ds(0, 7)], out_sem.at[1])
    await_bytes(qg.at[0, pl.ds(0, 7)], out_sem.at[2])
    await_bytes(lg.at[pl.ds(0, 31)], out_sem.at[3])
    await_bytes(qg.at[0], out_sem.at[4])
    await_bytes(xg.at[pl.ds(0, 30)], out_sem.at[5])
    await_bytes(xg.at[pl.ds(0, 16)], out_sem.at[6])
    await_bytes(xg.at[pl.ds(0, 14)], out_sem.at[7])
    await_bytes(outgoing.at[pl.ds(0, 15)], out_sem.at[8])
    await_bytes(msg, out_sem.at[9])
    await_bytes(mp.at[pl.ds(0, 14)], out_sem.at[10])


def on_device(
    q_latent, kv_latent, rope_key, q_latent_gain, kv_latent_gain, w_query, w_key, w_value, query_gain, key_gain,
    w_mix, tokens_b, norm_gain, expert_ids, route_weights, w_gate, w_up, w_down,
):
    base, shift = rope_tables()
    operands = (
        tokens_b, norm_gain, expert_ids.T, q_latent, kv_latent, rope_key, q_latent_gain, kv_latent_gain, query_gain,
        key_gain, jnp.asarray(base), jnp.asarray(shift), w_query.T, w_key, w_value, route_weights.T, w_gate, w_up, w_down,
        w_mix,
    )
    vmem = pl.BlockSpec(memory_space=pltpu.VMEM)
    hbm = pl.BlockSpec(memory_space=pl.ANY)
    dma = pltpu.SemaphoreType.DMA
    out = jax.ShapeDtypeStruct((48, 2048), BF16)
    results = pl.pallas_call(
        layer,
        out_shape=(out, out),
        in_specs=[hbm] * 20,
        out_specs=(vmem, vmem),
        scratch_shapes=[
            *[pltpu.VMEM(a.shape, a.dtype) for a in operands],
            pltpu.VMEM((256, 384), BF16),
            pltpu.VMEM((256, 256), BF16),
            pltpu.VMEM((2, 8, 48, 384), BF16),
            pltpu.VMEM((768, 256), BF16),
            pltpu.VMEM((768, 256), F32),
            pltpu.VMEM((32, 8, 48, 384), BF16),
            pltpu.VMEM((2, 48, 128), BF16),
            pltpu.VMEM((16, 16, 1024), BF16),
            pltpu.VMEM((16, 16, 1024), BF16),
            pltpu.VMEM((16, 16, 1024), BF16),
            pltpu.VMEM((32, HALF, 2048), BF16),
            pltpu.VMEM((32, HALF, 2048), BF16),
            pltpu.VMEM((16, HALF, 2048), BF16),
            pltpu.VMEM((7, HALF, 2048), BF16),
            pltpu.VMEM((7, HALF, 2048), BF16),
            pltpu.VMEM((32, 48, 1024), BF16),
            pltpu.VMEM((16, 48, 1024), BF16),
            pltpu.VMEM((7, 48, 1024), BF16),
            pltpu.VMEM((7, 48, 1024), BF16),
            dma((20,)),
            dma,
            dma((4,)),
            dma((3,)),
            dma,
            dma((4,)),
            dma((4, 4)),
            dma,
            dma((2,)),
            dma,
            dma((7,)),
            dma((7,)),
            dma((2,)),
            dma((7,)),
            dma((7,)),
            dma((16,)),
            dma((7,)),
            dma((7,)),
            dma,
            dma((7,)),
            dma((7,)),
            dma((11,)),
        ],
        compiler_params=pltpu.CompilerParams(
            collective_id=0, has_side_effects=True, vmem_limit_bytes=67_043_328
        ),
    )(*operands)
    return pl.pallas_call(hand_over, out_shape=(out, out), in_specs=[vmem] * 2, out_specs=(vmem, vmem))(*results)


def hand_over(mix_ref, expert_ref, mix_out, expert_out):
    mix_out[...] = mix_ref[...]
    expert_out[...] = expert_ref[...]


def solution(mesh):
    rows, whole = P(("ep", "tp"), None), P()
    in_specs = (
        rows, rows, rows, whole, whole, P(None, "tp"), P(None, "tp"), P(None, "tp"), whole, whole, P("tp", None), rows,
        whole, rows, rows, P("ep", None, "tp"), P("ep", None, "tp"), P("ep", "tp", None),
    )
    return jax.shard_map(on_device, mesh=mesh, in_specs=in_specs, out_specs=(rows, rows), check_vma=False)
```
